32 devices in a mesh: sp: 4 (over y, x), dp: 8 (over z, core).
Axes of the slice: x: 2, y: 2, z: 4, core: 2. Of those that a mesh axis runs over, the one named last changes fastest.
Arguments:
- tokens: bfloat16 [8, 1024, 2048], P('dp', 'sp'), may hold values from -6 to 6
- in_gain: float32 [2048], replicated, may hold values from 0.1 to 1.9
- query_weight: bfloat16 [2048, 2048], P('dp'), may hold values from -1 to 1
- key_weight: bfloat16 [2048, 512], P('dp'), may hold values from -1 to 1
- value_matrix: bfloat16 [2048, 512], P('dp'), may hold values from -0.125 to 0.125
- query_gain: float32 [128], replicated, may hold values from 1 to 6
- key_gain: float32 [128], replicated, may hold values from 1 to 6
- out_weight: bfloat16 [2048, 2048], P('dp'), may hold values from -0.125 to 0.125
- out_gain: float32 [2048], replicated, may hold values from 0.1 to 1.9
Outputs:
- mixed: bfloat16 [8, 1024, 2048], P('dp', 'sp')
The draws below stay inside these ranges and needn't reach their ends.
All inputs are finite; a program needn't handle non-finite values.
Results may differ from the reference program's by a relative error of at most 0.0055.
The reference program's roundings to bfloat16 on the way count: a program that leaves them out, or rounds other values in their place, can miss the bound.
Values may be sent and summed in bfloat16 or wider, within the bound.
A program may use at most 128 MiB of HBM per device.

```python
import jax
import jax.numpy as jnp
from jax import lax

MODEL_WIDTH = 2048
QUERY_HEAD_COUNT = 16
KEY_VALUE_HEADS = 4
HEAD_WIDTH = 128
GRID_W = 64
SEQUENCE_LENGTH = 1024
BATCH = 8


def query_for_group(key):
    return jax.random.truncated_normal(jax.random.fold_in(key, 101), -6.0, 6.0, (MODEL_WIDTH, QUERY_HEAD_COUNT * HEAD_WIDTH), jnp.float32) * MODEL_WIDTH ** (-0.5)


def draw_query_weight(key, part):
    return query_for_group(key).astype(jnp.bfloat16)


def draw_key_weight(key, part):
    complete_output = jax.random.truncated_normal(jax.random.fold_in(key, 401), -6.0, 6.0, (MODEL_WIDTH, KEY_VALUE_HEADS * HEAD_WIDTH), jnp.float32) * MODEL_WIDTH ** (-0.5)
    return complete_output.astype(jnp.bfloat16)


def draw_query_gain(key, part):
    return 1.6 * (1.0 + 0.18 * jax.random.uniform(jax.random.fold_in(key, 201), (HEAD_WIDTH,), jnp.float32, -1.0, 1.0))


def draw_key_gain(key, part):
    return 1.6 * (1.0 + 0.18 * jax.random.uniform(jax.random.fold_in(key, 301), (HEAD_WIDTH,), jnp.float32, -1.0, 1.0))


def level_of(key, dims, split, low, largest):
    def one(dim, shards_of):
        heights = jax.random.uniform(jax.random.fold_in(jax.random.fold_in(key, 6), dim), (shards_of,), jnp.float32, low / len(split), largest / len(split))
        return jnp.repeat(jnp.exp(heights), dims[dim] // shards_of).reshape((-1,) + (1,) * (len(dims) - dim - 1))

    level = one(*split[0])
    for cut in split[1:]:
        level = level * one(*cut)
    return level


def gaussian(rng, extent, deviation, reach, pieces=(), kind=jnp.bfloat16):
    drawn = deviation * jax.random.normal(rng, extent, jnp.float32)
    if pieces:
        drawn = drawn * level_of(rng, extent, pieces, -0.22, 0.18)
    return jnp.clip(drawn, -reach, reach).astype(kind)


def setup_inputs(seed: int = 0) -> dict:
    seeds = jax.random.split(jax.random.key(seed), 10)
    return {
        "tokens": gaussian(seeds[0], (BATCH, SEQUENCE_LENGTH, MODEL_WIDTH), 1.0, 6.0, ((0, 8), (1, 4))),
        "in_gain": jnp.clip(1.0 + 0.18 * jax.random.normal(seeds[1], (MODEL_WIDTH,), jnp.float32), 0.1, 1.9),
        "query_weight": draw_query_weight(jax.random.fold_in(seeds[9], 71), 0),
        "key_weight": draw_key_weight(jax.random.fold_in(seeds[9], 71), 0),
        "value_matrix": gaussian(seeds[4], (MODEL_WIDTH, KEY_VALUE_HEADS * HEAD_WIDTH), MODEL_WIDTH ** -0.5, 0.125, ((0, 8),)),
        "query_gain": draw_query_gain(jax.random.fold_in(seeds[9], 71), 0),
        "key_gain": draw_key_gain(jax.random.fold_in(seeds[9], 71), 0),
        "out_weight": gaussian(seeds[7], (QUERY_HEAD_COUNT * HEAD_WIDTH, MODEL_WIDTH), (QUERY_HEAD_COUNT * HEAD_WIDTH) ** -0.5, 0.125, ((0, 8),)),
        "out_gain": jnp.clip(1.0 + 0.18 * jax.random.normal(seeds[8], (MODEL_WIDTH,), jnp.float32), 0.1, 1.9),
    }


EPS = 1e-06
THETA = 10000.0

def norm_rows(row_data, gain_vec):
    return row_data * lax.rsqrt(lax.optimization_barrier(jnp.mean(row_data * row_data, axis=-1, keepdims=True)) + EPS) * gain_vec.astype(jnp.float32)

def rotate(head_data, positions):
    head_size = head_data.shape[-1]
    half_size = head_size // 2
    quarter = head_size // 4
    inverse_freq = THETA ** (-jnp.arange(quarter, dtype=jnp.float32) / quarter)
    row_angle = (positions // GRID_W).astype(jnp.float32)[:, None] * inverse_freq[None, :]
    col_angle = (positions % GRID_W).astype(jnp.float32)[:, None] * inverse_freq[None, :]

    def turn_half(half_part, angle):
        cosine = jnp.cos(angle)[:, None, :]
        sine_val = jnp.sin(angle)[:, None, :]
        first_part = half_part[..., :quarter]
        second_part = half_part[..., quarter:]
        return jnp.concatenate([first_part * cosine - second_part * sine_val, second_part * cosine + first_part * sine_val], axis=-1)
    return jnp.concatenate([turn_half(head_data[..., :half_size], row_angle), turn_half(head_data[..., half_size:], col_angle)], axis=-1)

def finish(projected, gain_vec, positions):
    row_count = projected.shape[0]
    heads_data = projected.reshape(row_count, -1, HEAD_WIDTH)
    heads_data = rotate(norm_rows(heads_data, gain_vec), positions)
    return heads_data.reshape(row_count, -1).astype(jnp.bfloat16)

def reference(tokens, in_gain, query_weight, key_weight, value_matrix, query_gain, key_gain, out_weight, out_gain):
    queries_per_group = QUERY_HEAD_COUNT // KEY_VALUE_HEADS
    rows_per_block = min(512, SEQUENCE_LENGTH)

    def per_sequence(sequence):
        float_rows = sequence.astype(jnp.float32)
        normed = norm_rows(float_rows, in_gain).astype(jnp.bfloat16)
        positions = jnp.arange(SEQUENCE_LENGTH, dtype=jnp.int32)
        query_rows = finish(jnp.dot(normed, query_weight, preferred_element_type=jnp.float32), query_gain, positions)
        key_matrix_rows = finish(jnp.dot(normed, key_weight, preferred_element_type=jnp.float32), key_gain, positions)
        value_rows = jnp.dot(normed, value_matrix, preferred_element_type=jnp.float32).astype(jnp.bfloat16)
        key_rows_float = key_matrix_rows.reshape(SEQUENCE_LENGTH, KEY_VALUE_HEADS, HEAD_WIDTH).astype(jnp.float32)
        value_rows_float = value_rows.reshape(SEQUENCE_LENGTH, KEY_VALUE_HEADS, HEAD_WIDTH).astype(jnp.float32)
        query_block_list = query_rows.reshape(SEQUENCE_LENGTH // rows_per_block, rows_per_block, KEY_VALUE_HEADS, queries_per_group, HEAD_WIDTH)

        def attend(query_block):
            scores = jnp.einsum('qegd,ked->egqk', query_block.astype(jnp.float32), key_rows_float) * HEAD_WIDTH ** (-0.5)
            shifted = scores - lax.optimization_barrier(jnp.max(scores, axis=-1, keepdims=True))
            raised = jnp.exp(shifted)
            weights = (raised / lax.optimization_barrier(jnp.sum(raised, axis=-1, keepdims=True))).astype(jnp.bfloat16)
            attended = jnp.einsum('egqk,ked->qegd', weights.astype(jnp.float32), value_rows_float)
            return attended.astype(jnp.bfloat16)
        attended = lax.map(attend, query_block_list).reshape(SEQUENCE_LENGTH, QUERY_HEAD_COUNT * HEAD_WIDTH)
        projected = jnp.dot(attended, out_weight, preferred_element_type=jnp.float32)
        return norm_rows(projected, out_gain).astype(jnp.bfloat16)
    return lax.map(per_sequence, tokens)
```

```python
import functools

import jax
import jax.numpy as jnp
import numpy as np
from jax import lax
from jax.experimental import pallas as pl
from jax.experimental.pallas import tpu as pltpu
from jax.sharding import PartitionSpec as P

QUERY_HEAD_COUNT = 16
KEY_VALUE_HEADS = 4
HEAD_WIDTH = 128
GRID_W = 64
EPS = 1e-06
THETA = 10000.0
MESH = pl.DeviceIdType.MESH
ANY = pl.BlockSpec(memory_space=pl.ANY)


def remote(src, dst, send_sem, recv_sem, device):
    return pltpu.make_async_remote_copy(
        src_ref=src, dst_ref=dst, send_sem=send_sem, recv_sem=recv_sem,
        device_id=device, device_id_type=MESH,
    )


def gather_kernel(
    parts, chips, q_width, kv_width, first_kv_of,
    x_ref, wq_ref, wk_ref, wv_ref, wo_ref, rows_ref, cols_ref, head_ref, tail_ref,
    stage, x_send, x_recv, own_sem, stage_sem,
    up_send, up_recv, down_send, down_recv, pair_send, pair_recv,
):
    sp, dp = lax.axis_index("sp"), lax.axis_index("dp")
    z, core = dp // 2, dp % 2
    partner = z * 2 + (1 - core)
    row_count = x_ref.shape[0]
    depth = stage.shape[0]
    square = parts == 4

    first_kv = first_kv_of(sp)
    loads = [
        pltpu.make_async_copy(
            wq_ref.at[:, pl.ds(pl.multiple_of(sp * q_width, 128), q_width)],
            stage.at[:, pl.ds(0, q_width)], stage_sem.at[0]),
        pltpu.make_async_copy(
            wk_ref.at[:, pl.ds(pl.multiple_of(first_kv * HEAD_WIDTH, 128), kv_width)],
            stage.at[:, pl.ds(q_width, kv_width)], stage_sem.at[1]),
        pltpu.make_async_copy(
            wv_ref.at[:, pl.ds(pl.multiple_of(first_kv * HEAD_WIDTH, 128), kv_width)],
            stage.at[:, pl.ds(q_width + kv_width, kv_width)], stage_sem.at[2]),
    ]
    for load in loads:
        load.start()

    barrier = pltpu.get_barrier_semaphore()
    if square:
        x_side = (sp // 2) * 2 + (1 - sp % 2)
        y_side = (1 - sp // 2) * 2 + sp % 2
        corner = (1 - sp // 2) * 2 + (1 - sp % 2)
        greeted = [x_side, y_side]
    else:
        greeted = [lax.rem(sp + i, parts) for i in range(1, parts)]
    for peer in greeted:
        pl.semaphore_signal(barrier, inc=1, device_id={"sp": peer, "dp": dp}, device_id_type=MESH)
    pl.semaphore_signal(barrier, inc=1, device_id={"sp": sp, "dp": partner}, device_id_type=MESH)

    @pl.when(z < chips - 1)
    def _():
        pl.semaphore_signal(barrier, inc=1, device_id={"sp": sp, "dp": dp + 2}, device_id_type=MESH)

    @pl.when(z > 0)
    def _():
        pl.semaphore_signal(barrier, inc=1, device_id={"sp": sp, "dp": dp - 2}, device_id_type=MESH)

    in_chain = (z + chips - 1) // chips + (2 * chips - 2 - z) // chips
    pl.semaphore_wait(barrier, len(greeted) + 1 + in_chain)

    def token_rows(owner, half=None):
        if half is None:
            return rows_ref.at[pl.ds(owner * row_count, row_count)]
        return rows_ref.at[pl.ds(owner * row_count + half * (row_count // 2), row_count // 2)]

    token_sends = []
    if square:
        for half_x, half_y in ((0, 1), (1, 0)):
            for slot, half, peer in ((0, half_x, x_side), (1, half_y, y_side)):
                copy = remote(
                    x_ref.at[pl.ds(half * (row_count // 2), row_count // 2)],
                    token_rows(sp, half), x_send.at[slot * 2 + half],
                    x_recv.at[slot * 2 + half], {"sp": peer, "dp": dp})
                copy.start()
                token_sends.append(copy)
    else:
        for i, peer in enumerate(greeted):
            copy = remote(
                x_ref, token_rows(sp), x_send.at[i], x_recv.at[i], {"sp": peer, "dp": dp})
            copy.start()
            token_sends.append(copy)
    own_rows = pltpu.make_async_copy(x_ref, token_rows(sp), own_sem.at[0])
    own_rows.start()
    split = head_ref.shape[1]
    out_head = wo_ref.at[:, pl.ds(0, split)]
    own_tail = pltpu.make_async_copy(
        wo_ref.at[:, pl.ds(split, tail_ref.shape[1])], tail_ref, own_sem.at[2])
    own_tail.start()

    for load in loads:
        load.wait()

    gathered = (cols_ref, head_ref)
    sources = (stage, out_head)

    def block(t, owner_z, owner_core):
        return gathered[t].at[pl.ds((owner_z * 2 + owner_core) * depth, depth)]

    def to_up(t, src, k):
        return remote(src, block(t, z - k, core), up_send.at[t, k], up_recv.at[t, k + 1],
                      {"sp": sp, "dp": dp + 2})

    def to_down(t, src, k):
        return remote(src, block(t, z + k, core), down_send.at[t, k], down_recv.at[t, k + 1],
                      {"sp": sp, "dp": dp - 2})

    def to_pair(t, src, owner_z):
        return remote(src, block(t, owner_z, core), pair_send.at[t, owner_z],
                      pair_recv.at[t, owner_z], {"sp": sp, "dp": partner})

    own_copies = []
    for t in range(2):
        @pl.when(z < chips - 1)
        def _():
            to_up(t, sources[t], 0).start()

        @pl.when(z > 0)
        def _():
            to_down(t, sources[t], 0).start()

        to_pair(t, sources[t], z).start()
        own = pltpu.make_async_copy(sources[t], block(t, z, core), own_sem.at[(1, 3)[t]])
        own.start()
        own_copies.append(own)

    if square:
        got_x = remote(x_ref.at[pl.ds(0, row_count // 2)], token_rows(x_side, 0),
                       x_send.at[0], x_recv.at[0], {"sp": x_side, "dp": dp})
        got_y = remote(x_ref.at[pl.ds(0, row_count // 2)], token_rows(y_side, 1),
                       x_send.at[3], x_recv.at[3], {"sp": y_side, "dp": dp})

    def relay_columns(t, k):
        @pl.when(z >= k)
        def _():
            source = block(t, z - k, core)
            remote(source, source, up_send.at[t, k], up_recv.at[t, k],
                   {"sp": sp, "dp": partner}).wait_recv()
            if k < chips - 1:
                @pl.when(z < chips - 1)
                def _():
                    to_up(t, source, k).start()
            to_pair(t, source, z - k).start()

        @pl.when(z + k <= chips - 1)
        def _():
            source = block(t, z + k, core)
            remote(source, source, down_send.at[t, k], down_recv.at[t, k],
                   {"sp": sp, "dp": partner}).wait_recv()
            if k < chips - 1:
                @pl.when(z > 0)
                def _():
                    to_down(t, source, k).start()
            to_pair(t, source, z + k).start()

    if chips > 1:
        relay_columns(0, 1)
    if square:
        got_x.wait_recv()
        relay_x = remote(token_rows(x_side, 0), token_rows(x_side, 0),
                         x_send.at[4], x_recv.at[4], {"sp": y_side, "dp": dp})
        relay_x.start()
        got_y.wait_recv()
        relay_y = remote(token_rows(y_side, 1), token_rows(y_side, 1),
                         x_send.at[5], x_recv.at[5], {"sp": x_side, "dp": dp})
        relay_y.start()
        token_sends += [relay_x, relay_y]
    for k in range(1, chips):
        if k > 1:
            relay_columns(0, k)
        relay_columns(1, k)

    for t in range(2):
        for owner_z in range(chips):
            source = block(t, owner_z, 1 - core)
            remote(source, source, pair_send.at[t, owner_z], pair_recv.at[t, owner_z],
                   {"sp": sp, "dp": partner}).wait_recv()
    if square:
        for owner, half, slot in (
            (x_side, 1, 1), (y_side, 0, 2), (corner, 0, 4), (corner, 1, 5)
        ):
            target = token_rows(owner, half)
            remote(target, target, x_send.at[slot], x_recv.at[slot],
                   {"sp": x_side, "dp": dp}).wait_recv()
    else:
        for i in range(parts - 1):
            target = token_rows(lax.rem(sp + parts - 1 - i, parts))
            remote(target, target, x_send.at[i], x_recv.at[i],
                   {"sp": greeted[0], "dp": dp}).wait_recv()
    for copy in token_sends:
        copy.wait_send()
    for t in range(2):
        for owner_z in range(chips):
            to_pair(t, sources[t], owner_z).wait_send()
        for k in range(chips - 1):
            @pl.when(jnp.logical_and(z < chips - 1, z >= k))
            def _():
                to_up(t, sources[t], k).wait_send()

            @pl.when(jnp.logical_and(z > 0, z + k <= chips - 1))
            def _():
                to_down(t, sources[t], k).wait_send()
    own_rows.wait()
    own_tail.wait()
    for own in own_copies:
        own.wait()


def gather(sequence, query_weight, key_weight, value_matrix, out_weight, parts, chips, q_width, kv_width, first_kv_of):
    depth, width = query_weight.shape[0], q_width + 2 * kv_width
    row_count, features = sequence.shape
    dma = pltpu.SemaphoreType.DMA
    chain = dma((2, chips + 1))
    split = out_weight.shape[1] // 2
    return pl.pallas_call(
        functools.partial(gather_kernel, parts, chips, q_width, kv_width, first_kv_of),
        out_shape=(
            jax.ShapeDtypeStruct((parts * row_count, features), jnp.bfloat16),
            jax.ShapeDtypeStruct((chips * 2 * depth, width), jnp.bfloat16),
            jax.ShapeDtypeStruct((chips * 2 * depth, split), jnp.bfloat16),
            jax.ShapeDtypeStruct((depth, out_weight.shape[1] - split), jnp.bfloat16),
        ),
        in_specs=[pl.BlockSpec(memory_space=pltpu.VMEM), ANY, ANY, ANY,
                  pl.BlockSpec(memory_space=pltpu.VMEM)],
        out_specs=(ANY, ANY, ANY, ANY),
        scratch_shapes=[
            pltpu.VMEM((depth, width), jnp.bfloat16),
            dma((max(6, parts),)), dma((max(6, parts),)), dma((4,)), dma((3,)),
            chain, chain, chain, chain, chain, chain,
        ],
        compiler_params=pltpu.CompilerParams(collective_id=0, has_side_effects=True),
        cost_estimate=pl.CostEstimate(flops=40_000_000_000, bytes_accessed=100_000_000, transcendentals=0),
        name="gather_rows_columns",
    )(sequence, query_weight, key_weight, value_matrix, out_weight)


def exchange_kernel(parts, a_ref, o_ref, send, recv, own_sem):
    sp, dp = lax.axis_index("sp"), lax.axis_index("dp")
    row_count = o_ref.shape[1]
    barrier = pltpu.get_barrier_semaphore()
    peers = [lax.rem(sp + i, parts) for i in range(1, parts)]
    for peer in peers:
        pl.semaphore_signal(barrier, inc=1, device_id={"sp": peer, "dp": dp}, device_id_type=MESH)
    pl.semaphore_wait(barrier, parts - 1)
    copies = []
    for i, peer in enumerate(peers):
        copy = remote(a_ref.at[pl.ds(peer * row_count, row_count)], o_ref.at[sp],
                      send.at[i], recv.at[i], {"sp": peer, "dp": dp})
        copy.start()
        copies.append(copy)
    own = pltpu.make_async_copy(a_ref.at[pl.ds(sp * row_count, row_count)], o_ref.at[sp], own_sem)
    own.start()
    for i in range(parts - 1):
        target = o_ref.at[lax.rem(sp + parts - 1 - i, parts)]
        remote(target, target, send.at[i], recv.at[i], {"sp": peers[0], "dp": dp}).wait_recv()
    for copy in copies:
        copy.wait_send()
    own.wait()


def exchange(attended, parts):
    length, width = attended.shape
    row_count = length // parts
    dma = pltpu.SemaphoreType.DMA
    return pl.pallas_call(
        functools.partial(exchange_kernel, parts),
        out_shape=jax.ShapeDtypeStruct((parts, row_count, width), jnp.bfloat16),
        in_specs=[pl.BlockSpec(memory_space=pltpu.VMEM)],
        out_specs=ANY,
        scratch_shapes=[dma((parts,)), dma((parts,)), dma],
        compiler_params=pltpu.CompilerParams(collective_id=1, has_side_effects=True),
        cost_estimate=pl.CostEstimate(flops=10_000_000_000, bytes_accessed=20_000_000, transcendentals=0),
        name="exchange_heads",
    )(attended)


def project_kernel(q_heads, kv_heads, x_ref, g_ref, w_ref, qg_ref, kg_ref, cos_ref, sin_ref,
                   q_ref, k_ref, v_ref):
    x = x_ref[...].astype(jnp.float32)
    scale = lax.rsqrt(jnp.mean(x * x, axis=-1, keepdims=True) + EPS)
    normed = (x * scale * g_ref[...]).astype(jnp.bfloat16)
    mixed = jnp.dot(normed, w_ref[...], preferred_element_type=jnp.float32)
    cosine, sine = cos_ref[...], sin_ref[...]
    lane = lax.broadcasted_iota(jnp.int32, cosine.shape, 1)
    first = lane % (HEAD_WIDTH // 2) < HEAD_WIDTH // 4

    def finish(head, gain):
        head = head * lax.rsqrt(jnp.mean(head * head, axis=-1, keepdims=True) + EPS) * gain
        other = jnp.where(first, pltpu.roll(head, HEAD_WIDTH - HEAD_WIDTH // 4, 1),
                          pltpu.roll(head, HEAD_WIDTH // 4, 1))
        return (head * cosine + other * sine).astype(jnp.bfloat16)

    for h in range(q_heads):
        span = slice(h * HEAD_WIDTH, (h + 1) * HEAD_WIDTH)
        q_ref[:, span] = finish(mixed[:, span], qg_ref[...])
    for h in range(kv_heads):
        span = slice(h * HEAD_WIDTH, (h + 1) * HEAD_WIDTH)
        start = (q_heads + h) * HEAD_WIDTH
        k_ref[:, span] = finish(mixed[:, start:start + HEAD_WIDTH], kg_ref[...])
    v_ref[...] = mixed[:, (q_heads + kv_heads) * HEAD_WIDTH:].astype(jnp.bfloat16)


def project(rows, in_gain, columns, query_gain, key_gain, cosine, sine, q_heads, kv_heads, row_block):
    length, features = rows.shape
    width = columns.shape[1]
    q_width, kv_width = q_heads * HEAD_WIDTH, kv_heads * HEAD_WIDTH
    whole = lambda shape: pl.BlockSpec(shape, lambda i: (0, 0))
    part = lambda size: pl.BlockSpec((row_block, size), lambda i: (i, 0))
    return pl.pallas_call(
        functools.partial(project_kernel, q_heads, kv_heads),
        grid=(length // row_block,),
        out_shape=tuple(jax.ShapeDtypeStruct((length, n), jnp.bfloat16) for n in (q_width, kv_width, kv_width)),
        in_specs=[part(features), whole((1, features)), whole((features, width)),
                  whole((1, HEAD_WIDTH)), whole((1, HEAD_WIDTH)), part(HEAD_WIDTH), part(HEAD_WIDTH)],
        out_specs=(part(q_width), part(kv_width), part(kv_width)),
        cost_estimate=pl.CostEstimate(flops=2 * length * features * width, bytes_accessed=9_000_000, transcendentals=0),
        name="project_heads",
    )(rows, in_gain[None], columns, query_gain[None], key_gain[None], cosine, sine)


def attend_kernel(group, q_ref, k_ref, v_ref, o_ref):
    factor = HEAD_WIDTH ** (-0.5) * float(np.log2(np.e))
    for h in range(q_ref.shape[1] // HEAD_WIDTH):
        span = slice(h * HEAD_WIDTH, (h + 1) * HEAD_WIDTH)
        shared = slice(h // group * HEAD_WIDTH, (h // group + 1) * HEAD_WIDTH)
        scores = lax.dot_general(q_ref[:, span], k_ref[:, shared], (((1,), (1,)), ((), ())),
                                 preferred_element_type=jnp.float32)
        top = jnp.max(scores, axis=-1, keepdims=True)
        raised = jnp.exp2((scores - top) * factor)
        weights = (raised * (1.0 / jnp.sum(raised, axis=-1, keepdims=True))).astype(jnp.bfloat16)
        o_ref[:, span] = jnp.dot(
            weights, v_ref[:, shared], preferred_element_type=jnp.float32).astype(jnp.bfloat16)


def attend(q, k, v, q_heads, kv_heads, row_block):
    length = q.shape[0]
    block = pl.BlockSpec((row_block, q.shape[1]), lambda i: (i, 0))
    keys = pl.BlockSpec(k.shape, lambda i: (0, 0))
    return pl.pallas_call(
        functools.partial(attend_kernel, q_heads // kv_heads),
        grid=(length // row_block,),
        out_shape=jax.ShapeDtypeStruct(q.shape, jnp.bfloat16),
        in_specs=[block, keys, keys],
        out_specs=block,
        cost_estimate=pl.CostEstimate(flops=4 * length * length * q_heads * HEAD_WIDTH,
                                      bytes_accessed=3_000_000, transcendentals=length * length * q_heads),
        name="attend_heads",
    )(q, k, v)


def output_kernel(a_ref, head_ref, tail_ref, g_ref, o_ref, total):
    step = pl.program_id(0)
    split = head_ref.shape[1]

    @pl.when(step == 0)
    def _():
        total[...] = jnp.zeros_like(total)

    total[:, :split] += jnp.dot(a_ref[0], head_ref[...], preferred_element_type=jnp.float32)
    total[:, split:] += jnp.dot(a_ref[0], tail_ref[...], preferred_element_type=jnp.float32)

    @pl.when(step == pl.num_programs(0) - 1)
    def _():
        x = total[...]
        scale = lax.rsqrt(jnp.mean(x * x, axis=-1, keepdims=True) + EPS)
        o_ref[...] = (x * scale * g_ref[...]).astype(jnp.bfloat16)


def output(returned, out_head, out_tail, out_gain):
    parts, row_count, width = returned.shape
    features = out_gain.shape[0]
    split = out_head.shape[1]
    return pl.pallas_call(
        output_kernel,
        grid=(parts,),
        out_shape=jax.ShapeDtypeStruct((row_count, features), jnp.bfloat16),
        in_specs=[pl.BlockSpec((1, row_count, width), lambda s: (s, 0, 0)),
                  pl.BlockSpec((width, split), lambda s: (s, 0)),
                  pl.BlockSpec((width, features - split), lambda s: (s, 0)),
                  pl.BlockSpec((1, features), lambda s: (0, 0))],
        out_specs=pl.BlockSpec((row_count, features), lambda s: (0, 0)),
        scratch_shapes=[pltpu.VMEM((row_count, features), jnp.float32)],
        cost_estimate=pl.CostEstimate(flops=2 * row_count * features * width * parts,
                                      bytes_accessed=10_000_000, transcendentals=0),
        name="output_rows",
    )(returned, out_head, out_tail, out_gain[None])


def fused_kernel(
    chips, q_width, kv_width,
    x_ref, wq_ref, wk_ref, wv_ref, wo_ref, ig_ref, qg_ref, kg_ref, cos_ref, sin_ref, og_ref,
    o_ref,
    xn, wkv, wqb, wob, q_buf, kv_buf, att, total, cosb, sinb,
    load_sem, tok_send, tok_recv, z_own, z_send, z_recv, y_send, y_recv, x_send, x_recv,
    kv_send, kv_recv, att_send, att_recv, p_send, p_recv,
):
    sp, dp = lax.axis_index("sp"), lax.axis_index("dp")
    z, core = dp // 2, dp % 2
    yi, xi = sp // 2, sp % 2
    R, F = x_ref.shape
    depth = wq_ref.shape[0]
    OD = wo_ref.shape[1]
    share = OD * 3 // 16 // 128 * 128
    rest = OD - 4 * share
    half = depth // 2
    width = 2 * q_width
    per = q_width // HEAD_WIDTH
    kv_per = kv_width // HEAD_WIDTH
    x_peer, y_peer = yi * 2 + (1 - xi), (1 - yi) * 2 + xi
    corner = (1 - yi) * 2 + (1 - xi)
    X = {"sp": x_peer, "dp": dp}
    Y = {"sp": y_peer, "dp": dp}
    PAIR = {"sp": sp, "dp": z * 2 + (1 - core)}
    others = chips - 1

    loads = []

    def load(src, dst):
        copy = pltpu.make_async_copy(src, dst, load_sem.at[len(loads)])
        copy.start()
        loads.append(copy)

    mine = pl.ds(pl.multiple_of(dp * depth, depth), depth)
    for j in range(2):
        at = pl.ds(pl.multiple_of((2 * xi + j) * kv_width, 128), kv_width)
        load(wk_ref.at[:, at], wkv.at[j, mine, pl.ds(0, kv_width)])
        load(wv_ref.at[:, at], wkv.at[j, mine, pl.ds(kv_width, kv_width)])
    for j in range(2):
        at = pl.ds(pl.multiple_of((2 * xi + j) * q_width, 128), q_width)
        load(wq_ref.at[:, at], wqb.at[j, mine])
    load(wo_ref, wob.at[mine])
    table = pl.ds(pl.multiple_of(yi * 2 * R, R), 2 * R)
    load(cos_ref.at[table], cosb)
    load(sin_ref.at[table], sinb)

    barrier = pltpu.get_barrier_semaphore()
    for peer in (X, Y, PAIR):
        pl.semaphore_signal(barrier, inc=1, device_id=peer, device_id_type=MESH)

    @pl.when(z < chips - 1)
    def _():
        pl.semaphore_signal(barrier, inc=1, device_id={"sp": sp, "dp": dp + 2}, device_id_type=MESH)

    @pl.when(z > 0)
    def _():
        pl.semaphore_signal(barrier, inc=1, device_id={"sp": sp, "dp": dp - 2}, device_id_type=MESH)

    in_chain = (z + others) // chips + (2 * others - z) // chips
    pl.semaphore_wait(barrier, 3 + in_chain)

    pending = []

    def send(ref, sems, recvs, index, peer, dst=None):
        copy = remote(ref, ref if dst is None else dst, sems.at[index], recvs.at[index], peer)
        copy.start()
        pending.append(copy)

    def arrived(ref, recvs, index):
        remote(ref, ref, p_send.at[0, 0], recvs.at[index], PAIR).wait_recv()

    def rows(owner, of, start=0, size=depth):
        return pl.ds(pl.multiple_of((owner * 2 + of) * depth, depth) + start, size)

    def quarter(owner, of, who, start=0, size=depth):
        return wob.at[rows(owner, of, start, size), pl.ds(pl.multiple_of(who * share, 128), share)]

    def block(t, owner, of, j=None):
        if t == 0:
            return wkv.at[yi if j is None else j, rows(owner, of)]
        if t == 1:
            return wqb.at[yi if j is None else j, rows(owner, of)]
        if t == 2:
            return quarter(owner, of, sp)
        return wob.at[rows(owner, of), pl.ds(4 * share, rest)]

    low = jnp.minimum(z, others - z)

    def owner_of(i):
        near = (i + 1) // 2
        paired = z - near if i % 2 else z + near
        alone = jnp.where(z > others - z, z - (i - low), z + (i - low))
        return jnp.where(i <= 2 * low, paired, alone)

    owners = [z] + [owner_of(i) for i in range(1, chips)]
    last_below = jnp.where(z == 0, 0, jnp.where(z <= others - z, 2 * z - 1, others))
    above = others - z
    last_above = jnp.where(above == 0, 0, jnp.where(above <= z, 2 * above, others))

    def start_own(t, up, now=None):
        ok = z < others if up else z > 0
        if now is not None:
            ok = jnp.logical_and(ok, (last_below if up else last_above) == now)

        @pl.when(ok)
        def _():
            ref = block(t, z, core)
            remote(ref, ref, z_own.at[t, int(up)], z_recv.at[t, z],
                   {"sp": sp, "dp": dp + (2 if up else -2)}).start()

    def to_pair(kind, owner, ref):
        remote(ref, ref, p_send.at[kind, owner], p_recv.at[kind, owner], PAIR).start()
        pending.append(remote(ref, ref, p_send.at[kind, owner], p_recv.at[kind, owner], PAIR))

    def relay_target(owner):
        step = jnp.where(owner < z, 1, -1)
        return jnp.logical_and(z + step >= 0, z + step < chips), {"sp": sp, "dp": dp + 2 * step}

    def from_z(t, i):
        owner = owners[i]
        ref = block(t, owner, core)
        arrived(ref, z_recv, (t, owner))
        ok, peer = relay_target(owner)

        @pl.when(ok)
        def _():
            remote(ref, ref, z_send.at[t, owner], z_recv.at[t, owner], peer).start()

        if t < 3:
            send(ref, y_send, y_recv, (t, owner), Y)
        if t == 2:
            send(ref, x_send, x_recv, (0, owner), X)
        to_pair(t, owner, ref)

    def from_y(t, i):
        owner = owners[i]
        if t < 2:
            ref = block(t, owner, core, 1 - yi)
        else:
            ref = quarter(owner, core, y_peer)
        arrived(ref, y_recv, (t, owner))
        if t == 2:
            send(quarter(owner, core, y_peer, 0, half), x_send, x_recv, (1, owner), X)
        to_pair(4 + t, owner, ref)

    def from_x(i):
        owner = owners[i]
        ref = quarter(owner, core, x_peer)
        arrived(ref, x_recv, (0, owner))
        send(quarter(owner, core, x_peer, half, half), y_send, y_recv, (3, owner), Y)
        to_pair(7, owner, ref)

    def from_corner(i):
        owner = owners[i]
        ref = quarter(owner, core, corner, 0, half)
        arrived(ref, x_recv, (1, owner))
        to_pair(8, owner, ref)
        ref = quarter(owner, core, corner, half, half)
        arrived(ref, y_recv, (3, owner))
        to_pair(9, owner, ref)

    def pair_has(kind, ref, owner):
        arrived(ref, p_recv, (kind, owner))

    send(x_ref, tok_send, tok_recv, 0, X, xn.at[pl.ds(pl.multiple_of(xi * R, R), R)])
    for copy in loads[:4]:
        copy.wait()
    start_own(0, True)
    start_own(0, False)
    to_pair(0, z, block(0, z, core))
    to_pair(4, z, block(0, z, core, 1 - yi))
    for copy in loads[4:6]:
        copy.wait()
    start_own(1, True)
    start_own(1, False)
    to_pair(1, z, block(1, z, core))
    to_pair(5, z, block(1, z, core, 1 - yi))
    for copy in loads[6:]:
        copy.wait()
    to_pair(2, z, wob.at[mine])

    def normalize(values, start):
        x = values.astype(jnp.float32)
        scale = lax.rsqrt(jnp.mean(x * x, axis=-1, keepdims=True) + EPS)
        xn[pl.ds(pl.multiple_of(start, R), R)] = (x * scale * ig_ref[...]).astype(jnp.bfloat16)

    def stage_own(t, now):
        start_own(t, True, now)
        start_own(t, False, now)

    normalize(x_ref[...], xi * R)
    stage_own(2, 0)
    for i in range(1, chips):
        from_z(0, i)
        if i > 1:
            from_y(1, i - 1)
        from_z(1, i)
        stage_own(2, i)
        from_y(0, i)

    lane = lax.broadcasted_iota(jnp.int32, (R, HEAD_WIDTH), 1)
    first = lane % (HEAD_WIDTH // 2) < HEAD_WIDTH // 4

    def finish(head, gain, cosine, sine):
        head = head * lax.rsqrt(jnp.mean(head * head, axis=-1, keepdims=True) + EPS) * gain
        other = jnp.where(first, pltpu.roll(head, HEAD_WIDTH - HEAD_WIDTH // 4, 1),
                          pltpu.roll(head, HEAD_WIDTH // 4, 1))
        return (head * cosine + other * sine).astype(jnp.bfloat16)

    def cut(values, h):
        return values[:, h * HEAD_WIDTH:(h + 1) * HEAD_WIDTH]

    for owner in range(chips):
        pair_has(0, block(0, owner, 1 - core), owner)
        pair_has(4, block(0, owner, 1 - core, 1 - yi), owner)

    def keys_values(who):
        local = pl.ds(pl.multiple_of(who * R, R), R)
        placed = pl.ds(pl.multiple_of((yi * 2 + who) * R, R), R)
        cosine, sine = cosb[local], sinb[local]
        for j in range(2):
            mixed = jnp.dot(xn[local], wkv[j], preferred_element_type=jnp.float32)
            for h in range(kv_per):
                start = j * kv_width + h * HEAD_WIDTH
                kv_buf[placed, start:start + HEAD_WIDTH] = finish(cut(mixed, h), kg_ref[...], cosine, sine)
            start = 2 * kv_width + j * kv_width
            kv_buf[placed, start:start + kv_width] = mixed[:, kv_width:].astype(jnp.bfloat16)
        return kv_buf.at[placed]

    send(keys_values(xi), kv_send, kv_recv, 0, Y)
    theirs = xn.at[pl.ds(pl.multiple_of((1 - xi) * R, R), R)]
    arrived(theirs, tok_recv, 0)
    normalize(theirs[...], (1 - xi) * R)
    send(keys_values(1 - xi), kv_send, kv_recv, 1, Y)

    def queries(j):
        @pl.loop(0, 2)
        def _(who):
            local = pl.ds(pl.multiple_of(who * R, R), R)
            cosine, sine = cosb[local], sinb[local]
            mixed = jnp.dot(xn[local], wqb[j], preferred_element_type=jnp.float32)
            for h in range(per):
                at = pl.ds(pl.multiple_of(j * q_width + h * HEAD_WIDTH, HEAD_WIDTH), HEAD_WIDTH)
                q_buf[local, at] = finish(cut(mixed, h), qg_ref[...], cosine, sine)

    stage_own(3, 0)
    from_z(2, 1)
    stage_own(3, 1)
    for owner in range(chips):
        pair_has(1, block(1, owner, 1 - core), owner)
    queries(yi)
    for i in range(2, chips):
        from_z(2, i)
        stage_own(3, i)
    from_y(1, others)
    for owner in range(chips):
        pair_has(5, block(1, owner, 1 - core, 1 - yi), owner)
    queries(1 - yi)
    from_x(1)
    for who in range(2):
        at = pl.ds(pl.multiple_of(((1 - yi) * 2 + (who + xi) % 2) * R, R), R)
        arrived(kv_buf.at[at], kv_recv, who)

    factor = HEAD_WIDTH ** (-0.5) * float(np.log2(np.e))
    couple = 2
    steps = 2 * per // couple

    def attend(step):
        turn = step % steps
        who = jnp.where(step < steps, 1 - xi, xi)
        local = pl.ds(pl.multiple_of(who * R, R), R)
        base = jnp.where(step < steps, 2 * width, xi * width) + turn * couple * HEAD_WIDTH
        for u in range(couple):
            head = turn * couple + u
            group = head // (per // kv_per)
            k_at = pl.ds(pl.multiple_of(group * HEAD_WIDTH, HEAD_WIDTH), HEAD_WIDTH)
            v_at = pl.ds(pl.multiple_of(2 * kv_width + group * HEAD_WIDTH, HEAD_WIDTH), HEAD_WIDTH)
            q_at = pl.ds(pl.multiple_of(head * HEAD_WIDTH, HEAD_WIDTH), HEAD_WIDTH)
            scores = lax.dot_general(q_buf[local, q_at], kv_buf[:, k_at], (((1,), (1,)), ((), ())),
                                     preferred_element_type=jnp.float32)
            top = jnp.max(scores, axis=-1, keepdims=True)
            raised = jnp.exp2((scores - top) * factor)
            weights = (raised * (1.0 / jnp.sum(raised, axis=-1, keepdims=True))).astype(jnp.bfloat16)
            att[:, pl.ds(pl.multiple_of(base + u * HEAD_WIDTH, HEAD_WIDTH), HEAD_WIDTH)] = jnp.dot(
                weights, kv_buf[:, v_at], preferred_element_type=jnp.float32).astype(jnp.bfloat16)

    def give(turn):
        size = couple * HEAD_WIDTH
        src = att.at[:, pl.ds(2 * width + turn * size, size)]
        dst = att.at[:, pl.ds(pl.multiple_of(xi * width + turn * size, 128), size)]
        send(src, att_send, att_recv, turn, X, dst)

    last = 2 * steps - 1
    timed = []
    for i in range(1, chips):
        if i > 1:
            timed.append((2 * i - 3, lambda i=i: from_x(i)))
        timed.append((3 * i - 1, lambda i=i: from_y(2, i)))
        timed.append((2 * i + 1, lambda i=i: from_z(3, i)))
        timed.append((last, lambda i=i: from_corner(i)))
    work = [[item for when, item in timed if min(when, last) == step] for step in range(2 * steps)]

    for step in range(2 * steps):
        attend(step)
        if step < steps:
            give(step)
        for item in work[step]:
            item()

    for turn in range(steps):
        size = couple * HEAD_WIDTH
        ref = att.at[:, pl.ds(pl.multiple_of((1 - xi) * width + turn * size, 128), size)]
        arrived(ref, att_recv, turn)
    for i in range(chips):
        owner = owners[i]
        if i == 0:
            pair_has(2, wob.at[rows(owner, 1 - core)], owner)
        else:
            pair_has(2, quarter(owner, 1 - core, sp), owner)
            pair_has(6, quarter(owner, 1 - core, y_peer), owner)
            pair_has(7, quarter(owner, 1 - core, x_peer), owner)
            pair_has(8, quarter(owner, 1 - core, corner, 0, half), owner)
            pair_has(9, quarter(owner, 1 - core, corner, half, half), owner)
            pair_has(3, block(3, owner, 1 - core), owner)

    tile = OD // 4

    @pl.loop(0, 4)
    def _(n):
        at = pl.ds(pl.multiple_of(n * tile, 128), tile)
        total[:, at] = jnp.dot(att[:, :2 * width], wob[:, at], preferred_element_type=jnp.float32)

    x = total[...]
    scale = lax.rsqrt(jnp.mean(x * x, axis=-1, keepdims=True) + EPS)
    o_ref[...] = (x * scale * og_ref[...]).astype(jnp.bfloat16)

    for copy in pending:
        copy.wait_send()
    for t in range(4):
        @pl.when(z < others)
        def _():
            ref = block(t, z, core)
            remote(ref, ref, z_own.at[t, 1], z_recv.at[t, z], PAIR).wait_send()

        @pl.when(z > 0)
        def _():
            ref = block(t, z, core)
            remote(ref, ref, z_own.at[t, 0], z_recv.at[t, z], PAIR).wait_send()

        for i in range(1, chips):
            owner = owners[i]
            ok, peer = relay_target(owner)

            @pl.when(ok)
            def _():
                ref = block(t, owner, core)
                remote(ref, ref, z_send.at[t, owner], z_recv.at[t, owner], peer).wait_send()


def fused(sequence, in_gain, query_weight, key_weight, value_matrix, query_gain, key_gain,
          out_weight, out_gain, cosine, sine, chips):
    row_count, features = sequence.shape
    q_width, kv_width = query_weight.shape[1] // 4, key_weight.shape[1] // 4
    columns = out_weight.shape[1]
    dma = pltpu.SemaphoreType.DMA
    vmem = pl.BlockSpec(memory_space=pltpu.VMEM)
    bf16, f32 = jnp.bfloat16, jnp.float32
    steps = q_width // HEAD_WIDTH
    return pl.pallas_call(
        functools.partial(fused_kernel, chips, q_width, kv_width),
        out_shape=jax.ShapeDtypeStruct((row_count, columns), bf16),
        in_specs=[vmem, ANY, ANY, ANY, ANY, vmem, vmem, vmem, ANY, ANY, vmem],
        out_specs=vmem,
        scratch_shapes=[
            pltpu.VMEM((2 * row_count, features), bf16),
            pltpu.VMEM((2, features, 2 * kv_width), bf16),
            pltpu.VMEM((2, features, q_width), bf16),
            pltpu.VMEM((out_weight.shape[0] * chips * 2, columns), bf16),
            pltpu.VMEM((2 * row_count, 2 * q_width), bf16),
            pltpu.VMEM((4 * row_count, 4 * kv_width), bf16),
            pltpu.VMEM((row_count, 6 * q_width), bf16),
            pltpu.VMEM((row_count, columns), f32),
            pltpu.VMEM((2 * row_count, HEAD_WIDTH), f32),
            pltpu.VMEM((2 * row_count, HEAD_WIDTH), f32),
            dma((9,)), dma((1,)), dma((1,)), dma((4, 2)), dma((4, chips)), dma((4, chips)),
            dma((4, chips)), dma((4, chips)), dma((2, chips)), dma((2, chips)),
            dma((2,)), dma((2,)), dma((steps,)), dma((steps,)),
            dma((10, chips)), dma((10, chips)),
        ],
        compiler_params=pltpu.CompilerParams(
            collective_id=0, has_side_effects=True, vmem_limit_bytes=60 * 1024 * 1024),
        cost_estimate=pl.CostEstimate(flops=10_000_000_000, bytes_accessed=10_000_000, transcendentals=0),
        name="attention_layer",
    )(sequence, query_weight, key_weight, value_matrix, out_weight, in_gain[None], query_gain[None],
      key_gain[None], cosine, sine, out_gain[None])


def rotation(length):
    quarter = HEAD_WIDTH // 4
    inverse_freq = (THETA ** (-np.arange(quarter, dtype=np.float32) / quarter)).astype(np.float32)

    def table(count):
        angle = (np.arange(count, dtype=np.float32)[:, None] * inverse_freq[None, :]).astype(np.float64)
        cosine, sine = np.cos(angle), np.sin(angle)
        return (np.concatenate([cosine, cosine], 1).astype(np.float32),
                np.concatenate([-sine, sine], 1).astype(np.float32))

    rows = -(-length // GRID_W)
    row_tables, col_tables = table(rows), table(GRID_W)
    half = HEAD_WIDTH // 2
    out = []
    for row, col in zip(row_tables, col_tables):
        row = np.broadcast_to(row[:, None, :], (rows, GRID_W, half))
        col = np.broadcast_to(col[None, :, :], (rows, GRID_W, half))
        full = np.concatenate([row, col], -1).reshape(rows * GRID_W, HEAD_WIDTH)
        out.append(jnp.asarray(full[:length]))
    return out


def on_device(parts, groups, tokens, in_gain, query_weight, key_weight, value_matrix,
              query_gain, key_gain, out_weight, out_gain):
    sequence = tokens[0]
    row_count = sequence.shape[0]
    q_heads = QUERY_HEAD_COUNT // parts
    kv_heads = max(1, KEY_VALUE_HEADS // parts)
    per_group = QUERY_HEAD_COUNT // KEY_VALUE_HEADS
    cosine, sine = rotation(parts * row_count)
    if parts == 4:
        return fused(sequence, in_gain, query_weight, key_weight, value_matrix, query_gain, key_gain,
                     out_weight, out_gain, cosine, sine, groups // 2)[None]
    rows, columns, out_head, own_tail = gather(
        sequence, query_weight, key_weight, value_matrix, out_weight, parts, groups // 2,
        q_heads * HEAD_WIDTH, kv_heads * HEAD_WIDTH, lambda sp: sp * q_heads // per_group)
    out_tail = lax.all_gather(own_tail, "dp", axis=0, tiled=True)
    q, k, v = project(rows, in_gain, columns, query_gain, key_gain, cosine, sine, q_heads, kv_heads, row_count)
    attended = attend(q, k, v, q_heads, kv_heads, row_count)
    returned = exchange(attended, parts)
    return output(returned, out_head, out_tail, out_gain)[None]


def solution(mesh):
    placed = (P("dp", "sp", None), P(), P("dp", None), P("dp", None), P("dp", None),
              P(), P(), P("dp", None), P())
    return jax.shard_map(
        functools.partial(on_device, mesh.shape["sp"], mesh.shape["dp"]),
        mesh=mesh, in_specs=placed, out_specs=P("dp", "sp", None), check_vma=False,
    )
```

```python
import functools

import jax
import jax.numpy as jnp
import numpy as np
from jax import lax
from jax.experimental import pallas as pl
from jax.experimental.pallas import tpu as pltpu
from jax.sharding import PartitionSpec as P

QUERY_HEAD_COUNT = 16
KEY_VALUE_HEADS = 4
HEAD_WIDTH = 128
GRID_W = 64
EPS = 1e-06
THETA = 10000.0
MESH = pl.DeviceIdType.MESH
ANY = pl.BlockSpec(memory_space=pl.ANY)


def remote(src, dst, send_sem, recv_sem, device):
    return pltpu.make_async_remote_copy(
        src_ref=src, dst_ref=dst, send_sem=send_sem, recv_sem=recv_sem,
        device_id=device, device_id_type=MESH,
    )


def gather_kernel(
    parts, chips, q_width, kv_width, first_kv_of,
    x_ref, wq_ref, wk_ref, wv_ref, wo_ref, rows_ref, cols_ref, head_ref, tail_ref,
    stage, x_send, x_recv, own_sem, stage_sem,
    up_send, up_recv, down_send, down_recv, pair_send, pair_recv,
):
    sp, dp = lax.axis_index("sp"), lax.axis_index("dp")
    z, core = dp // 2, dp % 2
    partner = z * 2 + (1 - core)
    row_count = x_ref.shape[0]
    depth = stage.shape[0]
    square = parts == 4

    first_kv = first_kv_of(sp)
    loads = [
        pltpu.make_async_copy(
            wq_ref.at[:, pl.ds(pl.multiple_of(sp * q_width, 128), q_width)],
            stage.at[:, pl.ds(0, q_width)], stage_sem.at[0]),
        pltpu.make_async_copy(
            wk_ref.at[:, pl.ds(pl.multiple_of(first_kv * HEAD_WIDTH, 128), kv_width)],
            stage.at[:, pl.ds(q_width, kv_width)], stage_sem.at[1]),
        pltpu.make_async_copy(
            wv_ref.at[:, pl.ds(pl.multiple_of(first_kv * HEAD_WIDTH, 128), kv_width)],
            stage.at[:, pl.ds(q_width + kv_width, kv_width)], stage_sem.at[2]),
    ]
    for load in loads:
        load.start()

    barrier = pltpu.get_barrier_semaphore()
    if square:
        x_side = (sp // 2) * 2 + (1 - sp % 2)
        y_side = (1 - sp // 2) * 2 + sp % 2
        corner = (1 - sp // 2) * 2 + (1 - sp % 2)
        greeted = [x_side, y_side]
    else:
        greeted = [lax.rem(sp + i, parts) for i in range(1, parts)]
    for peer in greeted:
        pl.semaphore_signal(barrier, inc=1, device_id={"sp": peer, "dp": dp}, device_id_type=MESH)
    pl.semaphore_signal(barrier, inc=1, device_id={"sp": sp, "dp": partner}, device_id_type=MESH)

    @pl.when(z < chips - 1)
    def _():
        pl.semaphore_signal(barrier, inc=1, device_id={"sp": sp, "dp": dp + 2}, device_id_type=MESH)

    @pl.when(z > 0)
    def _():
        pl.semaphore_signal(barrier, inc=1, device_id={"sp": sp, "dp": dp - 2}, device_id_type=MESH)

    in_chain = (z + chips - 1) // chips + (2 * chips - 2 - z) // chips
    pl.semaphore_wait(barrier, len(greeted) + 1 + in_chain)

    def token_rows(owner, half=None):
        if half is None:
            return rows_ref.at[pl.ds(owner * row_count, row_count)]
        return rows_ref.at[pl.ds(owner * row_count + half * (row_count // 2), row_count // 2)]

    token_sends = []
    if square:
        for half_x, half_y in ((0, 1), (1, 0)):
            for slot, half, peer in ((0, half_x, x_side), (1, half_y, y_side)):
                copy = remote(
                    x_ref.at[pl.ds(half * (row_count // 2), row_count // 2)],
                    token_rows(sp, half), x_send.at[slot * 2 + half],
                    x_recv.at[slot * 2 + half], {"sp": peer, "dp": dp})
                copy.start()
                token_sends.append(copy)
    else:
        for i, peer in enumerate(greeted):
            copy = remote(
                x_ref, token_rows(sp), x_send.at[i], x_recv.at[i], {"sp": peer, "dp": dp})
            copy.start()
            token_sends.append(copy)
    own_rows = pltpu.make_async_copy(x_ref, token_rows(sp), own_sem.at[0])
    own_rows.start()
    split = head_ref.shape[1]
    out_head = wo_ref.at[:, pl.ds(0, split)]
    own_tail = pltpu.make_async_copy(
        wo_ref.at[:, pl.ds(split, tail_ref.shape[1])], tail_ref, own_sem.at[2])
    own_tail.start()

    for load in loads:
        load.wait()

    gathered = (cols_ref, head_ref)
    sources = (stage, out_head)

    def block(t, owner_z, owner_core):
        return gathered[t].at[pl.ds((owner_z * 2 + owner_core) * depth, depth)]

    def to_up(t, src, k):
        return remote(src, block(t, z - k, core), up_send.at[t, k], up_recv.at[t, k + 1],
                      {"sp": sp, "dp": dp + 2})

    def to_down(t, src, k):
        return remote(src, block(t, z + k, core), down_send.at[t, k], down_recv.at[t, k + 1],
                      {"sp": sp, "dp": dp - 2})

    def to_pair(t, src, owner_z):
        return remote(src, block(t, owner_z, core), pair_send.at[t, owner_z],
                      pair_recv.at[t, owner_z], {"sp": sp, "dp": partner})

    own_copies = []
    for t in range(2):
        @pl.when(z < chips - 1)
        def _():
            to_up(t, sources[t], 0).start()

        @pl.when(z > 0)
        def _():
            to_down(t, sources[t], 0).start()

        to_pair(t, sources[t], z).start()
        own = pltpu.make_async_copy(sources[t], block(t, z, core), own_sem.at[(1, 3)[t]])
        own.start()
        own_copies.append(own)

    if square:
        got_x = remote(x_ref.at[pl.ds(0, row_count // 2)], token_rows(x_side, 0),
                       x_send.at[0], x_recv.at[0], {"sp": x_side, "dp": dp})
        got_y = remote(x_ref.at[pl.ds(0, row_count // 2)], token_rows(y_side, 1),
                       x_send.at[3], x_recv.at[3], {"sp": y_side, "dp": dp})

    def relay_columns(t, k):
        @pl.when(z >= k)
        def _():
            source = block(t, z - k, core)
            remote(source, source, up_send.at[t, k], up_recv.at[t, k],
                   {"sp": sp, "dp": partner}).wait_recv()
            if k < chips - 1:
                @pl.when(z < chips - 1)
                def _():
                    to_up(t, source, k).start()
            to_pair(t, source, z - k).start()

        @pl.when(z + k <= chips - 1)
        def _():
            source = block(t, z + k, core)
            remote(source, source, down_send.at[t, k], down_recv.at[t, k],
                   {"sp": sp, "dp": partner}).wait_recv()
            if k < chips - 1:
                @pl.when(z > 0)
                def _():
                    to_down(t, source, k).start()
            to_pair(t, source, z + k).start()

    if chips > 1:
        relay_columns(0, 1)
    if square:
        got_x.wait_recv()
        relay_x = remote(token_rows(x_side, 0), token_rows(x_side, 0),
                         x_send.at[4], x_recv.at[4], {"sp": y_side, "dp": dp})
        relay_x.start()
        got_y.wait_recv()
        relay_y = remote(token_rows(y_side, 1), token_rows(y_side, 1),
                         x_send.at[5], x_recv.at[5], {"sp": x_side, "dp": dp})
        relay_y.start()
        token_sends += [relay_x, relay_y]
    for k in range(1, chips):
        if k > 1:
            relay_columns(0, k)
        relay_columns(1, k)

    for t in range(2):
        for owner_z in range(chips):
            source = block(t, owner_z, 1 - core)
            remote(source, source, pair_send.at[t, owner_z], pair_recv.at[t, owner_z],
                   {"sp": sp, "dp": partner}).wait_recv()
    if square:
        for owner, half, slot in (
            (x_side, 1, 1), (y_side, 0, 2), (corner, 0, 4), (corner, 1, 5)
        ):
            target = token_rows(owner, half)
            remote(target, target, x_send.at[slot], x_recv.at[slot],
                   {"sp": x_side, "dp": dp}).wait_recv()
    else:
        for i in range(parts - 1):
            target = token_rows(lax.rem(sp + parts - 1 - i, parts))
            remote(target, target, x_send.at[i], x_recv.at[i],
                   {"sp": greeted[0], "dp": dp}).wait_recv()
    for copy in token_sends:
        copy.wait_send()
    for t in range(2):
        for owner_z in range(chips):
            to_pair(t, sources[t], owner_z).wait_send()
        for k in range(chips - 1):
            @pl.when(jnp.logical_and(z < chips - 1, z >= k))
            def _():
                to_up(t, sources[t], k).wait_send()

            @pl.when(jnp.logical_and(z > 0, z + k <= chips - 1))
            def _():
                to_down(t, sources[t], k).wait_send()
    own_rows.wait()
    own_tail.wait()
    for own in own_copies:
        own.wait()


def gather(sequence, query_weight, key_weight, value_matrix, out_weight, parts, chips, q_width, kv_width, first_kv_of):
    depth, width = query_weight.shape[0], q_width + 2 * kv_width
    row_count, features = sequence.shape
    dma = pltpu.SemaphoreType.DMA
    chain = dma((2, chips + 1))
    split = out_weight.shape[1] // 2
    return pl.pallas_call(
        functools.partial(gather_kernel, parts, chips, q_width, kv_width, first_kv_of),
        out_shape=(
            jax.ShapeDtypeStruct((parts * row_count, features), jnp.bfloat16),
            jax.ShapeDtypeStruct((chips * 2 * depth, width), jnp.bfloat16),
            jax.ShapeDtypeStruct((chips * 2 * depth, split), jnp.bfloat16),
            jax.ShapeDtypeStruct((depth, out_weight.shape[1] - split), jnp.bfloat16),
        ),
        in_specs=[pl.BlockSpec(memory_space=pltpu.VMEM), ANY, ANY, ANY,
                  pl.BlockSpec(memory_space=pltpu.VMEM)],
        out_specs=(ANY, ANY, ANY, ANY),
        scratch_shapes=[
            pltpu.VMEM((depth, width), jnp.bfloat16),
            dma((max(6, parts),)), dma((max(6, parts),)), dma((4,)), dma((3,)),
            chain, chain, chain, chain, chain, chain,
        ],
        compiler_params=pltpu.CompilerParams(collective_id=0, has_side_effects=True),
        cost_estimate=pl.CostEstimate(flops=40_000_000_000, bytes_accessed=100_000_000, transcendentals=0),
        name="gather_rows_columns",
    )(sequence, query_weight, key_weight, value_matrix, out_weight)


def exchange_kernel(parts, a_ref, o_ref, send, recv, own_sem):
    sp, dp = lax.axis_index("sp"), lax.axis_index("dp")
    row_count = o_ref.shape[1]
    barrier = pltpu.get_barrier_semaphore()
    peers = [lax.rem(sp + i, parts) for i in range(1, parts)]
    for peer in peers:
        pl.semaphore_signal(barrier, inc=1, device_id={"sp": peer, "dp": dp}, device_id_type=MESH)
    pl.semaphore_wait(barrier, parts - 1)
    copies = []
    for i, peer in enumerate(peers):
        copy = remote(a_ref.at[pl.ds(peer * row_count, row_count)], o_ref.at[sp],
                      send.at[i], recv.at[i], {"sp": peer, "dp": dp})
        copy.start()
        copies.append(copy)
    own = pltpu.make_async_copy(a_ref.at[pl.ds(sp * row_count, row_count)], o_ref.at[sp], own_sem)
    own.start()
    for i in range(parts - 1):
        target = o_ref.at[lax.rem(sp + parts - 1 - i, parts)]
        remote(target, target, send.at[i], recv.at[i], {"sp": peers[0], "dp": dp}).wait_recv()
    for copy in copies:
        copy.wait_send()
    own.wait()


def exchange(attended, parts):
    length, width = attended.shape
    row_count = length // parts
    dma = pltpu.SemaphoreType.DMA
    return pl.pallas_call(
        functools.partial(exchange_kernel, parts),
        out_shape=jax.ShapeDtypeStruct((parts, row_count, width), jnp.bfloat16),
        in_specs=[pl.BlockSpec(memory_space=pltpu.VMEM)],
        out_specs=ANY,
        scratch_shapes=[dma((parts,)), dma((parts,)), dma],
        compiler_params=pltpu.CompilerParams(collective_id=1, has_side_effects=True),
        cost_estimate=pl.CostEstimate(flops=10_000_000_000, bytes_accessed=20_000_000, transcendentals=0),
        name="exchange_heads",
    )(attended)


def project_kernel(q_heads, kv_heads, x_ref, g_ref, w_ref, qg_ref, kg_ref, cos_ref, sin_ref,
                   q_ref, k_ref, v_ref):
    x = x_ref[...].astype(jnp.float32)
    scale = lax.rsqrt(jnp.mean(x * x, axis=-1, keepdims=True) + EPS)
    normed = (x * scale * g_ref[...]).astype(jnp.bfloat16)
    mixed = jnp.dot(normed, w_ref[...], preferred_element_type=jnp.float32)
    cosine, sine = cos_ref[...], sin_ref[...]
    lane = lax.broadcasted_iota(jnp.int32, cosine.shape, 1)
    first = lane % (HEAD_WIDTH // 2) < HEAD_WIDTH // 4

    def finish(head, gain):
        head = head * lax.rsqrt(jnp.mean(head * head, axis=-1, keepdims=True) + EPS) * gain
        other = jnp.where(first, pltpu.roll(head, HEAD_WIDTH - HEAD_WIDTH // 4, 1),
                          pltpu.roll(head, HEAD_WIDTH // 4, 1))
        return (head * cosine + other * sine).astype(jnp.bfloat16)

    for h in range(q_heads):
        span = slice(h * HEAD_WIDTH, (h + 1) * HEAD_WIDTH)
        q_ref[:, span] = finish(mixed[:, span], qg_ref[...])
    for h in range(kv_heads):
        span = slice(h * HEAD_WIDTH, (h + 1) * HEAD_WIDTH)
        start = (q_heads + h) * HEAD_WIDTH
        k_ref[:, span] = finish(mixed[:, start:start + HEAD_WIDTH], kg_ref[...])
    v_ref[...] = mixed[:, (q_heads + kv_heads) * HEAD_WIDTH:].astype(jnp.bfloat16)


def project(rows, in_gain, columns, query_gain, key_gain, cosine, sine, q_heads, kv_heads, row_block):
    length, features = rows.shape
    width = columns.shape[1]
    q_width, kv_width = q_heads * HEAD_WIDTH, kv_heads * HEAD_WIDTH
    whole = lambda shape: pl.BlockSpec(shape, lambda i: (0, 0))
    part = lambda size: pl.BlockSpec((row_block, size), lambda i: (i, 0))
    return pl.pallas_call(
        functools.partial(project_kernel, q_heads, kv_heads),
        grid=(length // row_block,),
        out_shape=tuple(jax.ShapeDtypeStruct((length, n), jnp.bfloat16) for n in (q_width, kv_width, kv_width)),
        in_specs=[part(features), whole((1, features)), whole((features, width)),
                  whole((1, HEAD_WIDTH)), whole((1, HEAD_WIDTH)), part(HEAD_WIDTH), part(HEAD_WIDTH)],
        out_specs=(part(q_width), part(kv_width), part(kv_width)),
        cost_estimate=pl.CostEstimate(flops=2 * length * features * width, bytes_accessed=9_000_000, transcendentals=0),
        name="project_heads",
    )(rows, in_gain[None], columns, query_gain[None], key_gain[None], cosine, sine)


def attend_kernel(group, q_ref, k_ref, v_ref, o_ref):
    factor = HEAD_WIDTH ** (-0.5) * float(np.log2(np.e))
    for h in range(q_ref.shape[1] // HEAD_WIDTH):
        span = slice(h * HEAD_WIDTH, (h + 1) * HEAD_WIDTH)
        shared = slice(h // group * HEAD_WIDTH, (h // group + 1) * HEAD_WIDTH)
        scores = lax.dot_general(q_ref[:, span], k_ref[:, shared], (((1,), (1,)), ((), ())),
                                 preferred_element_type=jnp.float32)
        top = jnp.max(scores, axis=-1, keepdims=True)
        raised = jnp.exp2((scores - top) * factor)
        weights = (raised * (1.0 / jnp.sum(raised, axis=-1, keepdims=True))).astype(jnp.bfloat16)
        o_ref[:, span] = jnp.dot(
            weights, v_ref[:, shared], preferred_element_type=jnp.float32).astype(jnp.bfloat16)


def attend(q, k, v, q_heads, kv_heads, row_block):
    length = q.shape[0]
    block = pl.BlockSpec((row_block, q.shape[1]), lambda i: (i, 0))
    keys = pl.BlockSpec(k.shape, lambda i: (0, 0))
    return pl.pallas_call(
        functools.partial(attend_kernel, q_heads // kv_heads),
        grid=(length // row_block,),
        out_shape=jax.ShapeDtypeStruct(q.shape, jnp.bfloat16),
        in_specs=[block, keys, keys],
        out_specs=block,
        cost_estimate=pl.CostEstimate(flops=4 * length * length * q_heads * HEAD_WIDTH,
                                      bytes_accessed=3_000_000, transcendentals=length * length * q_heads),
        name="attend_heads",
    )(q, k, v)


def output_kernel(a_ref, head_ref, tail_ref, g_ref, o_ref, total):
    step = pl.program_id(0)
    split = head_ref.shape[1]

    @pl.when(step == 0)
    def _():
        total[...] = jnp.zeros_like(total)

    total[:, :split] += jnp.dot(a_ref[0], head_ref[...], preferred_element_type=jnp.float32)
    total[:, split:] += jnp.dot(a_ref[0], tail_ref[...], preferred_element_type=jnp.float32)

    @pl.when(step == pl.num_programs(0) - 1)
    def _():
        x = total[...]
        scale = lax.rsqrt(jnp.mean(x * x, axis=-1, keepdims=True) + EPS)
        o_ref[...] = (x * scale * g_ref[...]).astype(jnp.bfloat16)


def output(returned, out_head, out_tail, out_gain):
    parts, row_count, width = returned.shape
    features = out_gain.shape[0]
    split = out_head.shape[1]
    return pl.pallas_call(
        output_kernel,
        grid=(parts,),
        out_shape=jax.ShapeDtypeStruct((row_count, features), jnp.bfloat16),
        in_specs=[pl.BlockSpec((1, row_count, width), lambda s: (s, 0, 0)),
                  pl.BlockSpec((width, split), lambda s: (s, 0)),
                  pl.BlockSpec((width, features - split), lambda s: (s, 0)),
                  pl.BlockSpec((1, features), lambda s: (0, 0))],
        out_specs=pl.BlockSpec((row_count, features), lambda s: (0, 0)),
        scratch_shapes=[pltpu.VMEM((row_count, features), jnp.float32)],
        cost_estimate=pl.CostEstimate(flops=2 * row_count * features * width * parts,
                                      bytes_accessed=10_000_000, transcendentals=0),
        name="output_rows",
    )(returned, out_head, out_tail, out_gain[None])


def fused_kernel(
    chips, q_width, kv_width,
    x_in, wq_ref, wk_ref, wv_ref, wo_ref, ig_in, qg_in, kg_in, cos_ref, sin_ref, og_in,
    o_ref,
    x_ref, ig_ref, qg_ref, kg_ref, og_ref, xn, wkv, wqb, wob, q_buf, kv_buf, att, total, out, cosb, sinb,
    load_sem, tok_send, tok_recv, z_own, z_send, z_recv, y_send, y_recv, x_send, x_recv,
    kv_send, kv_recv, att_send, att_recv, p_send, p_recv, own_send, own_recv,
):
    sp, dp = lax.axis_index("sp"), lax.axis_index("dp")
    z, core = dp // 2, dp % 2
    yi, xi = sp // 2, sp % 2
    R, F = x_in.shape
    depth = wq_ref.shape[0]
    OD = wo_ref.shape[1]
    wide, narrow, rest = OD // 8, OD // 16, OD // 4
    shared = depth // 2
    width = 2 * q_width
    per = q_width // HEAD_WIDTH
    kv_per = kv_width // HEAD_WIDTH
    x_peer, y_peer = yi * 2 + (1 - xi), (1 - yi) * 2 + xi
    corner = (1 - yi) * 2 + (1 - xi)
    X = {"sp": x_peer, "dp": dp}
    Y = {"sp": y_peer, "dp": dp}
    PAIR = {"sp": sp, "dp": z * 2 + (1 - core)}
    others = chips - 1

    barrier = pltpu.get_barrier_semaphore()
    for peer in (X, Y, PAIR):
        pl.semaphore_signal(barrier, inc=1, device_id=peer, device_id_type=MESH)

    @pl.when(z < chips - 1)
    def _():
        pl.semaphore_signal(barrier, inc=1, device_id={"sp": sp, "dp": dp + 2}, device_id_type=MESH)

    @pl.when(z > 0)
    def _():
        pl.semaphore_signal(barrier, inc=1, device_id={"sp": sp, "dp": dp - 2}, device_id_type=MESH)

    loads = []

    def load(src, dst):
        copy = pltpu.make_async_copy(src, dst, load_sem.at[len(loads)])
        copy.start()
        loads.append(copy)

    mine = pl.ds(pl.multiple_of(dp * depth, depth), depth)
    load(x_in, x_ref)
    for j in range(2):
        at = pl.ds(pl.multiple_of((2 * xi + j) * kv_width, 128), kv_width)
        load(wk_ref.at[:, at], wkv.at[j, mine, pl.ds(0, kv_width)])
        load(wv_ref.at[:, at], wkv.at[j, mine, pl.ds(kv_width, kv_width)])
    for j in range(2):
        at = pl.ds(pl.multiple_of((2 * xi + j) * q_width, 128), q_width)
        load(wq_ref.at[:, at], wqb.at[j, mine])
    load(wo_ref, wob.at[mine])
    table = pl.ds(pl.multiple_of(yi * 2 * R, R), 2 * R)
    load(cos_ref.at[table], cosb)
    load(sin_ref.at[table], sinb)
    for source, target in ((ig_in, ig_ref), (qg_in, qg_ref), (kg_in, kg_ref), (og_in, og_ref)):
        load(source, target)

    in_chain = (z + others) // chips + (2 * others - z) // chips
    pl.semaphore_wait(barrier, 3 + in_chain)

    def send(make, sems, recvs, index, peer, make_dst=None):
        slot = index[0] if isinstance(index, tuple) else 0
        for src, dst in zip(make(), (make_dst or make)()):
            remote(src, dst, sems.at[slot], recvs.at[index], peer).start()

    def sent(ref, sems, slot):
        remote(ref, ref, sems.at[slot], p_recv.at[0], PAIR).wait_send()

    def arrived(ref, recvs, index):
        remote(ref, ref, p_send.at[0], recvs.at[index], PAIR).wait_recv()

    def rows(owner, of, start=0, size=depth):
        return pl.ds(pl.multiple_of((owner * 2 + of) * depth, depth) + start, size)

    def quarter(owner, of, who, a=0, b=2):
        broad = wob.at[rows(owner, of, a * depth // 2, (b - a) * depth // 2),
                       pl.ds(pl.multiple_of(who * wide, 128), wide)]
        slim = wob.at[rows(owner, of, a * shared // 2, (b - a) * shared // 2),
                      pl.ds(pl.multiple_of(4 * wide + who * narrow, 128), narrow)]
        return [broad, slim]

    def quarters(times, a=0, b=2):
        return wob.at[:times * (b - a) * (depth // 2 + shared // 4), :wide]

    def rests(times):
        return wob.at[:times * (2 * depth - shared), :rest]

    def block(t, owner, of, j=None):
        if t == 0:
            return [wkv.at[yi if j is None else j, rows(owner, of)]]
        if t == 1:
            return [wqb.at[yi if j is None else j, rows(owner, of)]]
        if t == 2:
            return quarter(owner, of, sp)
        return [wob.at[rows(owner, of), pl.ds(OD - rest, rest)],
                wob.at[rows(owner, of, shared, depth - shared), pl.ds(4 * wide, 4 * narrow)]]

    def bulk(t):
        if t == 0:
            return wkv.at[0, :depth]
        if t == 1:
            return wqb.at[0, :depth]
        return quarters(1) if t == 2 else rests(1)

    low = jnp.minimum(z, others - z)

    def owner_of(i):
        near = (i + 1) // 2
        paired = z - near if i % 2 else z + near
        alone = jnp.where(z > others - z, z - (i - low), z + (i - low))
        return jnp.where(i <= 2 * low, paired, alone)

    owners = [z] + [owner_of(i) for i in range(1, chips)]
    last_below = jnp.where(z == 0, 0, jnp.where(z <= others - z, 2 * z - 1, others))
    above = others - z
    last_above = jnp.where(above == 0, 0, jnp.where(above <= z, 2 * above, others))

    def start_own(t, up, now=None):
        ok = z < others if up else z > 0
        if now is not None:
            ok = jnp.logical_and(ok, (last_below if up else last_above) == now)

        @pl.when(ok)
        def _():
            for ref in block(t, z, core):
                remote(ref, ref, z_own.at[t, int(up)], z_recv.at[t, z],
                       {"sp": sp, "dp": dp + (2 if up else -2)}).start()

    def to_pair(kind, refs):
        group = {0: 0, 4: 0, 1: 1, 5: 2, 2: 3, 7: 4, 6: 5, 8: 6, 9: 6, 3: 7}[kind]
        for ref in refs:
            remote(ref, ref, p_send.at[group], p_recv.at[group], PAIR).start()

    def pair_refs():
        half = wqb.at[0, :F // 2]
        return [wkv.at[0], half, half] + [quarters(others)] * 4 + [rests(others)]

    def pair_wait(group):
        ref = pair_refs()[group]
        remote(ref, ref, p_send.at[group], p_recv.at[group], PAIR).wait_recv()

    def relay_target(owner):
        step = jnp.where(owner < z, 1, -1)
        return jnp.logical_and(z + step >= 0, z + step < chips), {"sp": sp, "dp": dp + 2 * step}

    def from_z(t, i):
        owner = owners[i]
        arrived(bulk(t), z_recv, (t, owner))
        ok, peer = relay_target(owner)

        @pl.when(ok)
        def _():
            for ref in block(t, owner, core):
                remote(ref, ref, z_send.at[t, owner], z_recv.at[t, owner], peer).start()

        def make():
            return block(t, owner, core)

        if t < 2:
            send(make, y_send, y_recv, (t, owner), Y)
        if t == 2:
            send(make, x_send, x_recv, (0, owner), X)
        to_pair(t, make())

    def share_y(i):
        owner = owners[i]
        send(lambda: block(2, owner, core), y_send, y_recv, (2, owner), Y)

    def from_y(t, i):
        owner = owners[i]
        arrived(bulk(t), y_recv, (t, owner))
        if t == 2:
            send(lambda: quarter(owner, core, y_peer, 0, 1), x_send, x_recv, (1, owner), X)
            to_pair(6, quarter(owner, core, y_peer))
        else:
            to_pair(4 + t, block(t, owner, core, 1 - yi))

    def from_x(i):
        owner = owners[i]
        arrived(bulk(2), x_recv, (0, owner))
        send(lambda: quarter(owner, core, x_peer, 1, 2), y_send, y_recv, (3, owner), Y)
        to_pair(7, quarter(owner, core, x_peer))

    def corner_x(i):
        owner = owners[i]
        arrived(quarters(1, 0, 1), x_recv, (1, owner))
        to_pair(8, quarter(owner, core, corner, 0, 1))

    def corner_y(i):
        owner = owners[i]
        arrived(quarters(1, 1, 2), y_recv, (3, owner))
        to_pair(9, quarter(owner, core, corner, 1, 2))

    for copy in loads[:5]:
        copy.wait()
    send(lambda: [x_ref], tok_send, tok_recv, 0, X, lambda: [xn.at[pl.ds(pl.multiple_of(xi * R, R), R)]])
    start_own(0, True)
    start_own(0, False)
    to_pair(0, block(0, z, core))
    to_pair(4, block(0, z, core, 1 - yi))
    for copy in loads[5:7]:
        copy.wait()
    start_own(1, True)
    start_own(1, False)
    to_pair(1, block(1, z, core))
    to_pair(5, block(1, z, core, 1 - yi))
    for copy in loads[7:]:
        copy.wait()
    remote(wob.at[mine], wob.at[mine], own_send.at[0], own_recv.at[0], PAIR).start()

    def normalize(values, start):
        x = values.astype(jnp.float32)
        scale = lax.rsqrt(jnp.mean(x * x, axis=-1, keepdims=True) + EPS)
        xn[pl.ds(pl.multiple_of(start, R), R)] = (x * scale * ig_ref[...]).astype(jnp.bfloat16)

    def stage_own(t, now):
        start_own(t, True, now)
        start_own(t, False, now)

    inner = low > 0

    def quarter_stage(i, early):
        @pl.when(inner if early else jnp.logical_not(inner))
        def _():
            from_z(2, i)
            stage_own(3, i)

    def rest_stage(i, early):
        @pl.when(inner if early else jnp.logical_not(inner))
        def _():
            from_z(3, i)

    def quarter_late(i):
        quarter_stage(i, False)
        share_y(i)

    normalize(x_ref[...], xi * R)
    stage_own(2, 0)
    stage_own(3, 0)
    for i in range(1, chips):
        from_z(0, i)
        if i > 2:
            from_y(1, i - 2)
        if i > 1:
            from_y(0, i - 1)
        from_z(1, i)
        stage_own(2, i)

    for i in range(1, chips):
        quarter_stage(i, True)
    lane = lax.broadcasted_iota(jnp.int32, (R, HEAD_WIDTH), 1)
    first = lane % (HEAD_WIDTH // 2) < HEAD_WIDTH // 4

    def finish(head, gain, cosine, sine):
        head = head * lax.rsqrt(jnp.mean(head * head, axis=-1, keepdims=True) + EPS) * gain
        other = jnp.where(first, pltpu.roll(head, HEAD_WIDTH - HEAD_WIDTH // 4, 1),
                          pltpu.roll(head, HEAD_WIDTH // 4, 1))
        return (head * cosine + other * sine).astype(jnp.bfloat16)

    def cut(values, h):
        return values[:, h * HEAD_WIDTH:(h + 1) * HEAD_WIDTH]

    if chips > 2:
        from_y(1, others - 1)
    from_y(0, others)
    pair_wait(0)

    def keys_values(turn, who):
        local = pl.ds(pl.multiple_of(who * R, R), R)
        placed = pl.ds(pl.multiple_of((yi * 2 + who) * R, R), R)
        cosine, sine = cosb[local], sinb[local]
        for j in range(2):
            mixed = jnp.dot(xn[local], wkv[j], preferred_element_type=jnp.float32)
            for h in range(kv_per):
                start = j * kv_width + h * HEAD_WIDTH
                kv_buf[placed, start:start + HEAD_WIDTH] = finish(cut(mixed, h), kg_ref[...], cosine, sine)
            start = 2 * kv_width + j * kv_width
            kv_buf[placed, start:start + kv_width] = mixed[:, kv_width:].astype(jnp.bfloat16)
        send(lambda: [kv_buf.at[pl.ds(pl.multiple_of((yi * 2 + who) * R, R), R)]],
             kv_send, kv_recv, turn, Y)

    keys_values(0, xi)
    theirs = xn.at[pl.ds(pl.multiple_of((1 - xi) * R, R), R)]
    arrived(theirs, tok_recv, 0)
    normalize(theirs[...], (1 - xi) * R)
    keys_values(1, 1 - xi)

    def queries(j):
        @pl.loop(0, 2)
        def _(who):
            local = pl.ds(pl.multiple_of(who * R, R), R)
            cosine, sine = cosb[local], sinb[local]
            mixed = jnp.dot(xn[local], wqb[j], preferred_element_type=jnp.float32)
            for h in range(per):
                at = pl.ds(pl.multiple_of(j * q_width + h * HEAD_WIDTH, HEAD_WIDTH), HEAD_WIDTH)
                q_buf[local, at] = finish(cut(mixed, h), qg_ref[...], cosine, sine)

    quarter_late(1)
    pair_wait(1)
    queries(yi)
    for i in range(min(2, others), 0, -1):
        rest_stage(i, True)
    from_y(1, others)
    pair_wait(2)
    queries(1 - yi)
    for i in range(2, chips):
        quarter_late(i)
    from_x(1)
    for i in range(3, chips):
        rest_stage(i, True)
    for who in range(2):
        at = pl.ds(pl.multiple_of(((1 - yi) * 2 + (who + xi) % 2) * R, R), R)
        arrived(kv_buf.at[at], kv_recv, who)

    factor = HEAD_WIDTH ** (-0.5) * float(np.log2(np.e))
    couple = 2
    steps = 2 * per // couple

    def attend(step):
        turn = step % steps
        who = 1 - xi if step < steps else xi
        local = pl.ds(pl.multiple_of(who * R, R), R)
        place = 2 if step < steps else xi
        base = turn * couple * HEAD_WIDTH
        for u in range(couple):
            head = turn * couple + u
            group = head // (per // kv_per)
            k_at = pl.ds(pl.multiple_of(group * HEAD_WIDTH, HEAD_WIDTH), HEAD_WIDTH)
            v_at = pl.ds(pl.multiple_of(2 * kv_width + group * HEAD_WIDTH, HEAD_WIDTH), HEAD_WIDTH)
            q_at = pl.ds(pl.multiple_of(head * HEAD_WIDTH, HEAD_WIDTH), HEAD_WIDTH)
            scores = lax.dot_general(q_buf[local, q_at], kv_buf[:, k_at], (((1,), (1,)), ((), ())),
                                     preferred_element_type=jnp.float32)
            top = jnp.max(scores, axis=-1, keepdims=True)
            raised = jnp.exp2((scores - top) * factor)
            weights = (raised * (1.0 / jnp.sum(raised, axis=-1, keepdims=True))).astype(jnp.bfloat16)
            att[place, :, base + u * HEAD_WIDTH:base + (u + 1) * HEAD_WIDTH] = jnp.dot(
                weights, kv_buf[:, v_at], preferred_element_type=jnp.float32).astype(jnp.bfloat16)

    def give(turn):
        size = couple * HEAD_WIDTH
        send(lambda: [att.at[2, :, pl.ds(turn * size, size)]], att_send, att_recv, 0, X,
             lambda: [att.at[xi, :, pl.ds(turn * size, size)]])

    last = 2 * steps - 1
    timed = []
    for i in range(1, chips):
        if i > 1:
            timed.append((2 * i - 3, lambda i=i: from_x(i)))
        timed.append((3 * i - 1, lambda i=i: from_y(2, i)))
        timed.append((3 * i - 1, lambda i=i: rest_stage(i, False)))
    work = [[item for when, item in timed if min(when, last) == step] for step in range(2 * steps)]

    for step in range(2 * steps):
        attend(step)
        if step < steps:
            give(step)
        for item in work[step]:
            item()

    def project(zones, mine):
        half = xi if mine else 1 - xi
        left = att[half]
        deep = pl.ds(pl.multiple_of(half * width, width), width)
        for at in zones:
            part = jnp.dot(left, wob[deep, at], preferred_element_type=jnp.float32)
            total[:, at] = part if mine else total[:, at] + part

    def zone(who):
        return pl.ds(pl.multiple_of(who * wide, 128), wide)

    arrived(wob.at[rows(z, 1 - core)], own_recv, 0)
    pair_wait(3)
    pair_wait(4)
    project([zone(sp), zone(x_peer)], True)
    pair_wait(5)
    pair_wait(7)
    project([zone(y_peer), pl.ds(OD - rest, rest)], True)
    for i in range(1, chips):
        corner_y(i)
        corner_x(i)
    arrived(att.at[1 - xi], att_recv, 0)
    project([pl.ds(OD - rest, rest), zone(sp), zone(x_peer), zone(y_peer)], False)
    pair_wait(6)
    late = [zone(corner), pl.ds(4 * wide, 4 * narrow)]
    project(late, True)
    project(late, False)

    chunk = R // 4
    stores = []
    for n in range(4):
        at = pl.ds(n * chunk, chunk)
        x = total[at]
        scale = lax.rsqrt(jnp.mean(x * x, axis=-1, keepdims=True) + EPS)
        out[at] = (x * scale * og_ref[...]).astype(jnp.bfloat16)
        store = pltpu.make_async_copy(out.at[at], o_ref.at[at], load_sem.at[n])
        store.start()
        stores.append(store)

    count = others * depth
    sent(x_ref, tok_send, 0)
    sent(wkv.at[0, :count], y_send, 0)
    sent(wqb.at[0, :count], y_send, 1)
    sent(quarters(others), y_send, 2)
    sent(quarters(others, 1, 2), y_send, 3)
    sent(quarters(others), x_send, 0)
    sent(quarters(others, 0, 1), x_send, 1)
    sent(kv_buf.at[:2 * R], kv_send, 0)
    sent(att.at[2], att_send, 0)
    for group, ref in enumerate(pair_refs()):
        sent(ref, p_send, group)
    sent(wob.at[mine], own_send, 0)
    for t in range(4):
        @pl.when(z < others)
        def _():
            ref = bulk(t)
            remote(ref, ref, z_own.at[t, 1], z_recv.at[t, z], PAIR).wait_send()

        @pl.when(z > 0)
        def _():
            ref = bulk(t)
            remote(ref, ref, z_own.at[t, 0], z_recv.at[t, z], PAIR).wait_send()

        for i in range(1, chips):
            owner = owners[i]
            ok, peer = relay_target(owner)

            @pl.when(ok)
            def _():
                ref = bulk(t)
                remote(ref, ref, z_send.at[t, owner], z_recv.at[t, owner], peer).wait_send()

    for store in stores:
        store.wait()


def fused(sequence, in_gain, query_weight, key_weight, value_matrix, query_gain, key_gain,
          out_weight, out_gain, cosine, sine, chips):
    row_count, features = sequence.shape
    q_width, kv_width = query_weight.shape[1] // 4, key_weight.shape[1] // 4
    columns = out_weight.shape[1]
    dma = pltpu.SemaphoreType.DMA
    bf16, f32 = jnp.bfloat16, jnp.float32
    return pl.pallas_call(
        functools.partial(fused_kernel, chips, q_width, kv_width),
        out_shape=jax.ShapeDtypeStruct((row_count, columns), bf16),
        in_specs=[ANY] * 11,
        out_specs=ANY,
        scratch_shapes=[
            pltpu.VMEM((row_count, features), bf16),
            pltpu.VMEM((1, features), f32),
            pltpu.VMEM((1, HEAD_WIDTH), f32),
            pltpu.VMEM((1, HEAD_WIDTH), f32),
            pltpu.VMEM((1, columns), f32),
            pltpu.VMEM((2 * row_count, features), bf16),
            pltpu.VMEM((2, features, 2 * kv_width), bf16),
            pltpu.VMEM((2, features, q_width), bf16),
            pltpu.VMEM((out_weight.shape[0] * chips * 2, columns), bf16),
            pltpu.VMEM((2 * row_count, 2 * q_width), bf16),
            pltpu.VMEM((4 * row_count, 4 * kv_width), bf16),
            pltpu.VMEM((3, row_count, 2 * q_width), bf16),
            pltpu.VMEM((row_count, columns), f32),
            pltpu.VMEM((row_count, columns), bf16),
            pltpu.VMEM((2 * row_count, HEAD_WIDTH), f32),
            pltpu.VMEM((2 * row_count, HEAD_WIDTH), f32),
            dma((14,)), dma((1,)), dma((1,)), dma((4, 2)), dma((4, chips)), dma((4, chips)),
            dma((4,)), dma((4, chips)), dma((2,)), dma((2, chips)),
            dma((1,)), dma((2,)), dma((1,)), dma((1,)), dma((8,)), dma((8,)), dma((1,)), dma((1,)),
        ],
        compiler_params=pltpu.CompilerParams(
            collective_id=0, has_side_effects=True, vmem_limit_bytes=60 * 1024 * 1024),
        cost_estimate=pl.CostEstimate(flops=10_000_000_000, bytes_accessed=10_000_000, transcendentals=0),
        name="attention_layer",
    )(sequence, query_weight, key_weight, value_matrix, out_weight, in_gain[None], query_gain[None],
      key_gain[None], cosine, sine, out_gain[None])


def rotation(length):
    quarter = HEAD_WIDTH // 4
    inverse_freq = (THETA ** (-np.arange(quarter, dtype=np.float32) / quarter)).astype(np.float32)

    def table(count):
        angle = (np.arange(count, dtype=np.float32)[:, None] * inverse_freq[None, :]).astype(np.float64)
        cosine, sine = np.cos(angle), np.sin(angle)
        return (np.concatenate([cosine, cosine], 1).astype(np.float32),
                np.concatenate([-sine, sine], 1).astype(np.float32))

    rows = -(-length // GRID_W)
    row_tables, col_tables = table(rows), table(GRID_W)
    half = HEAD_WIDTH // 2
    out = []
    for row, col in zip(row_tables, col_tables):
        row = np.broadcast_to(row[:, None, :], (rows, GRID_W, half))
        col = np.broadcast_to(col[None, :, :], (rows, GRID_W, half))
        full = np.concatenate([row, col], -1).reshape(rows * GRID_W, HEAD_WIDTH)
        out.append(jnp.asarray(full[:length]))
    return out


def on_device(parts, groups, tokens, in_gain, query_weight, key_weight, value_matrix,
              query_gain, key_gain, out_weight, out_gain):
    sequence = tokens[0]
    row_count = sequence.shape[0]
    q_heads = QUERY_HEAD_COUNT // parts
    kv_heads = max(1, KEY_VALUE_HEADS // parts)
    per_group = QUERY_HEAD_COUNT // KEY_VALUE_HEADS
    cosine, sine = rotation(parts * row_count)
    if parts == 4:
        return fused(sequence, in_gain, query_weight, key_weight, value_matrix, query_gain, key_gain,
                     out_weight, out_gain, cosine, sine, groups // 2)[None]
    rows, columns, out_head, own_tail = gather(
        sequence, query_weight, key_weight, value_matrix, out_weight, parts, groups // 2,
        q_heads * HEAD_WIDTH, kv_heads * HEAD_WIDTH, lambda sp: sp * q_heads // per_group)
    out_tail = lax.all_gather(own_tail, "dp", axis=0, tiled=True)
    q, k, v = project(rows, in_gain, columns, query_gain, key_gain, cosine, sine, q_heads, kv_heads, row_count)
    attended = attend(q, k, v, q_heads, kv_heads, row_count)
    returned = exchange(attended, parts)
    return output(returned, out_head, out_tail, out_gain)[None]


def solution(mesh):
    placed = (P("dp", "sp", None), P(), P("dp", None), P("dp", None), P("dp", None),
              P(), P(), P("dp", None), P())
    return jax.shard_map(
        functools.partial(on_device, mesh.shape["sp"], mesh.shape["dp"]),
        mesh=mesh, in_specs=placed, out_specs=P("dp", "sp", None), check_vma=False,
    )
```

```python
import functools

import jax
import jax.numpy as jnp
import numpy as np
from jax import lax
from jax.experimental import pallas as pl
from jax.experimental.pallas import tpu as pltpu
from jax.sharding import PartitionSpec as P

QUERY_HEAD_COUNT = 16
KEY_VALUE_HEADS = 4
HEAD_WIDTH = 128
GRID_W = 64
EPS = 1e-06
THETA = 10000.0
MESH = pl.DeviceIdType.MESH
ANY = pl.BlockSpec(memory_space=pl.ANY)


def remote(src, dst, send_sem, recv_sem, device):
    return pltpu.make_async_remote_copy(
        src_ref=src, dst_ref=dst, send_sem=send_sem, recv_sem=recv_sem,
        device_id=device, device_id_type=MESH,
    )


def gather_kernel(
    parts, chips, q_width, kv_width, first_kv_of,
    x_ref, wq_ref, wk_ref, wv_ref, wo_ref, rows_ref, cols_ref, head_ref, tail_ref,
    stage, x_send, x_recv, own_sem, stage_sem,
    up_send, up_recv, down_send, down_recv, pair_send, pair_recv,
):
    sp, dp = lax.axis_index("sp"), lax.axis_index("dp")
    z, core = dp // 2, dp % 2
    partner = z * 2 + (1 - core)
    row_count = x_ref.shape[0]
    depth = stage.shape[0]
    square = parts == 4

    first_kv = first_kv_of(sp)
    loads = [
        pltpu.make_async_copy(
            wq_ref.at[:, pl.ds(pl.multiple_of(sp * q_width, 128), q_width)],
            stage.at[:, pl.ds(0, q_width)], stage_sem.at[0]),
        pltpu.make_async_copy(
            wk_ref.at[:, pl.ds(pl.multiple_of(first_kv * HEAD_WIDTH, 128), kv_width)],
            stage.at[:, pl.ds(q_width, kv_width)], stage_sem.at[1]),
        pltpu.make_async_copy(
            wv_ref.at[:, pl.ds(pl.multiple_of(first_kv * HEAD_WIDTH, 128), kv_width)],
            stage.at[:, pl.ds(q_width + kv_width, kv_width)], stage_sem.at[2]),
    ]
    for load in loads:
        load.start()

    barrier = pltpu.get_barrier_semaphore()
    if square:
        x_side = (sp // 2) * 2 + (1 - sp % 2)
        y_side = (1 - sp // 2) * 2 + sp % 2
        corner = (1 - sp // 2) * 2 + (1 - sp % 2)
        greeted = [x_side, y_side]
    else:
        greeted = [lax.rem(sp + i, parts) for i in range(1, parts)]
    for peer in greeted:
        pl.semaphore_signal(barrier, inc=1, device_id={"sp": peer, "dp": dp}, device_id_type=MESH)
    pl.semaphore_signal(barrier, inc=1, device_id={"sp": sp, "dp": partner}, device_id_type=MESH)

    @pl.when(z < chips - 1)
    def _():
        pl.semaphore_signal(barrier, inc=1, device_id={"sp": sp, "dp": dp + 2}, device_id_type=MESH)

    @pl.when(z > 0)
    def _():
        pl.semaphore_signal(barrier, inc=1, device_id={"sp": sp, "dp": dp - 2}, device_id_type=MESH)

    in_chain = (z + chips - 1) // chips + (2 * chips - 2 - z) // chips
    pl.semaphore_wait(barrier, len(greeted) + 1 + in_chain)

    def token_rows(owner, half=None):
        if half is None:
            return rows_ref.at[pl.ds(owner * row_count, row_count)]
        return rows_ref.at[pl.ds(owner * row_count + half * (row_count // 2), row_count // 2)]

    token_sends = []
    if square:
        for half_x, half_y in ((0, 1), (1, 0)):
            for slot, half, peer in ((0, half_x, x_side), (1, half_y, y_side)):
                copy = remote(
                    x_ref.at[pl.ds(half * (row_count // 2), row_count // 2)],
                    token_rows(sp, half), x_send.at[slot * 2 + half],
                    x_recv.at[slot * 2 + half], {"sp": peer, "dp": dp})
                copy.start()
                token_sends.append(copy)
    else:
        for i, peer in enumerate(greeted):
            copy = remote(
                x_ref, token_rows(sp), x_send.at[i], x_recv.at[i], {"sp": peer, "dp": dp})
            copy.start()
            token_sends.append(copy)
    own_rows = pltpu.make_async_copy(x_ref, token_rows(sp), own_sem.at[0])
    own_rows.start()
    split = head_ref.shape[1]
    out_head = wo_ref.at[:, pl.ds(0, split)]
    own_tail = pltpu.make_async_copy(
        wo_ref.at[:, pl.ds(split, tail_ref.shape[1])], tail_ref, own_sem.at[2])
    own_tail.start()

    for load in loads:
        load.wait()

    gathered = (cols_ref, head_ref)
    sources = (stage, out_head)

    def block(t, owner_z, owner_core):
        return gathered[t].at[pl.ds((owner_z * 2 + owner_core) * depth, depth)]

    def to_up(t, src, k):
        return remote(src, block(t, z - k, core), up_send.at[t, k], up_recv.at[t, k + 1],
                      {"sp": sp, "dp": dp + 2})

    def to_down(t, src, k):
        return remote(src, block(t, z + k, core), down_send.at[t, k], down_recv.at[t, k + 1],
                      {"sp": sp, "dp": dp - 2})

    def to_pair(t, src, owner_z):
        return remote(src, block(t, owner_z, core), pair_send.at[t, owner_z],
                      pair_recv.at[t, owner_z], {"sp": sp, "dp": partner})

    own_copies = []
    for t in range(2):
        @pl.when(z < chips - 1)
        def _():
            to_up(t, sources[t], 0).start()

        @pl.when(z > 0)
        def _():
            to_down(t, sources[t], 0).start()

        to_pair(t, sources[t], z).start()
        own = pltpu.make_async_copy(sources[t], block(t, z, core), own_sem.at[(1, 3)[t]])
        own.start()
        own_copies.append(own)

    if square:
        got_x = remote(x_ref.at[pl.ds(0, row_count // 2)], token_rows(x_side, 0),
                       x_send.at[0], x_recv.at[0], {"sp": x_side, "dp": dp})
        got_y = remote(x_ref.at[pl.ds(0, row_count // 2)], token_rows(y_side, 1),
                       x_send.at[3], x_recv.at[3], {"sp": y_side, "dp": dp})

    def relay_columns(t, k):
        @pl.when(z >= k)
        def _():
            source = block(t, z - k, core)
            remote(source, source, up_send.at[t, k], up_recv.at[t, k],
                   {"sp": sp, "dp": partner}).wait_recv()
            if k < chips - 1:
                @pl.when(z < chips - 1)
                def _():
                    to_up(t, source, k).start()
            to_pair(t, source, z - k).start()

        @pl.when(z + k <= chips - 1)
        def _():
            source = block(t, z + k, core)
            remote(source, source, down_send.at[t, k], down_recv.at[t, k],
                   {"sp": sp, "dp": partner}).wait_recv()
            if k < chips - 1:
                @pl.when(z > 0)
                def _():
                    to_down(t, source, k).start()
            to_pair(t, source, z + k).start()

    if chips > 1:
        relay_columns(0, 1)
    if square:
        got_x.wait_recv()
        relay_x = remote(token_rows(x_side, 0), token_rows(x_side, 0),
                         x_send.at[4], x_recv.at[4], {"sp": y_side, "dp": dp})
        relay_x.start()
        got_y.wait_recv()
        relay_y = remote(token_rows(y_side, 1), token_rows(y_side, 1),
                         x_send.at[5], x_recv.at[5], {"sp": x_side, "dp": dp})
        relay_y.start()
        token_sends += [relay_x, relay_y]
    for k in range(1, chips):
        if k > 1:
            relay_columns(0, k)
        relay_columns(1, k)

    for t in range(2):
        for owner_z in range(chips):
            source = block(t, owner_z, 1 - core)
            remote(source, source, pair_send.at[t, owner_z], pair_recv.at[t, owner_z],
                   {"sp": sp, "dp": partner}).wait_recv()
    if square:
        for owner, half, slot in (
            (x_side, 1, 1), (y_side, 0, 2), (corner, 0, 4), (corner, 1, 5)
        ):
            target = token_rows(owner, half)
            remote(target, target, x_send.at[slot], x_recv.at[slot],
                   {"sp": x_side, "dp": dp}).wait_recv()
    else:
        for i in range(parts - 1):
            target = token_rows(lax.rem(sp + parts - 1 - i, parts))
            remote(target, target, x_send.at[i], x_recv.at[i],
                   {"sp": greeted[0], "dp": dp}).wait_recv()
    for copy in token_sends:
        copy.wait_send()
    for t in range(2):
        for owner_z in range(chips):
            to_pair(t, sources[t], owner_z).wait_send()
        for k in range(chips - 1):
            @pl.when(jnp.logical_and(z < chips - 1, z >= k))
            def _():
                to_up(t, sources[t], k).wait_send()

            @pl.when(jnp.logical_and(z > 0, z + k <= chips - 1))
            def _():
                to_down(t, sources[t], k).wait_send()
    own_rows.wait()
    own_tail.wait()
    for own in own_copies:
        own.wait()


def gather(sequence, query_weight, key_weight, value_matrix, out_weight, parts, chips, q_width, kv_width, first_kv_of):
    depth, width = query_weight.shape[0], q_width + 2 * kv_width
    row_count, features = sequence.shape
    dma = pltpu.SemaphoreType.DMA
    chain = dma((2, chips + 1))
    split = out_weight.shape[1] // 2
    return pl.pallas_call(
        functools.partial(gather_kernel, parts, chips, q_width, kv_width, first_kv_of),
        out_shape=(
            jax.ShapeDtypeStruct((parts * row_count, features), jnp.bfloat16),
            jax.ShapeDtypeStruct((chips * 2 * depth, width), jnp.bfloat16),
            jax.ShapeDtypeStruct((chips * 2 * depth, split), jnp.bfloat16),
            jax.ShapeDtypeStruct((depth, out_weight.shape[1] - split), jnp.bfloat16),
        ),
        in_specs=[pl.BlockSpec(memory_space=pltpu.VMEM), ANY, ANY, ANY,
                  pl.BlockSpec(memory_space=pltpu.VMEM)],
        out_specs=(ANY, ANY, ANY, ANY),
        scratch_shapes=[
            pltpu.VMEM((depth, width), jnp.bfloat16),
            dma((max(6, parts),)), dma((max(6, parts),)), dma((4,)), dma((3,)),
            chain, chain, chain, chain, chain, chain,
        ],
        compiler_params=pltpu.CompilerParams(collective_id=0, has_side_effects=True),
        cost_estimate=pl.CostEstimate(flops=40_000_000_000, bytes_accessed=100_000_000, transcendentals=0),
        name="gather_rows_columns",
    )(sequence, query_weight, key_weight, value_matrix, out_weight)


def exchange_kernel(parts, a_ref, o_ref, send, recv, own_sem):
    sp, dp = lax.axis_index("sp"), lax.axis_index("dp")
    row_count = o_ref.shape[1]
    barrier = pltpu.get_barrier_semaphore()
    peers = [lax.rem(sp + i, parts) for i in range(1, parts)]
    for peer in peers:
        pl.semaphore_signal(barrier, inc=1, device_id={"sp": peer, "dp": dp}, device_id_type=MESH)
    pl.semaphore_wait(barrier, parts - 1)
    copies = []
    for i, peer in enumerate(peers):
        copy = remote(a_ref.at[pl.ds(peer * row_count, row_count)], o_ref.at[sp],
                      send.at[i], recv.at[i], {"sp": peer, "dp": dp})
        copy.start()
        copies.append(copy)
    own = pltpu.make_async_copy(a_ref.at[pl.ds(sp * row_count, row_count)], o_ref.at[sp], own_sem)
    own.start()
    for i in range(parts - 1):
        target = o_ref.at[lax.rem(sp + parts - 1 - i, parts)]
        remote(target, target, send.at[i], recv.at[i], {"sp": peers[0], "dp": dp}).wait_recv()
    for copy in copies:
        copy.wait_send()
    own.wait()


def exchange(attended, parts):
    length, width = attended.shape
    row_count = length // parts
    dma = pltpu.SemaphoreType.DMA
    return pl.pallas_call(
        functools.partial(exchange_kernel, parts),
        out_shape=jax.ShapeDtypeStruct((parts, row_count, width), jnp.bfloat16),
        in_specs=[pl.BlockSpec(memory_space=pltpu.VMEM)],
        out_specs=ANY,
        scratch_shapes=[dma((parts,)), dma((parts,)), dma],
        compiler_params=pltpu.CompilerParams(collective_id=1, has_side_effects=True),
        cost_estimate=pl.CostEstimate(flops=10_000_000_000, bytes_accessed=20_000_000, transcendentals=0),
        name="exchange_heads",
    )(attended)


def project_kernel(q_heads, kv_heads, x_ref, g_ref, w_ref, qg_ref, kg_ref, cos_ref, sin_ref,
                   q_ref, k_ref, v_ref):
    x = x_ref[...].astype(jnp.float32)
    scale = lax.rsqrt(jnp.mean(x * x, axis=-1, keepdims=True) + EPS)
    normed = (x * scale * g_ref[...]).astype(jnp.bfloat16)
    mixed = jnp.dot(normed, w_ref[...], preferred_element_type=jnp.float32)
    cosine, sine = cos_ref[...], sin_ref[...]
    lane = lax.broadcasted_iota(jnp.int32, cosine.shape, 1)
    first = lane % (HEAD_WIDTH // 2) < HEAD_WIDTH // 4

    def finish(head, gain):
        head = head * lax.rsqrt(jnp.mean(head * head, axis=-1, keepdims=True) + EPS) * gain
        other = jnp.where(first, pltpu.roll(head, HEAD_WIDTH - HEAD_WIDTH // 4, 1),
                          pltpu.roll(head, HEAD_WIDTH // 4, 1))
        return (head * cosine + other * sine).astype(jnp.bfloat16)

    for h in range(q_heads):
        span = slice(h * HEAD_WIDTH, (h + 1) * HEAD_WIDTH)
        q_ref[:, span] = finish(mixed[:, span], qg_ref[...])
    for h in range(kv_heads):
        span = slice(h * HEAD_WIDTH, (h + 1) * HEAD_WIDTH)
        start = (q_heads + h) * HEAD_WIDTH
        k_ref[:, span] = finish(mixed[:, start:start + HEAD_WIDTH], kg_ref[...])
    v_ref[...] = mixed[:, (q_heads + kv_heads) * HEAD_WIDTH:].astype(jnp.bfloat16)


def project(rows, in_gain, columns, query_gain, key_gain, cosine, sine, q_heads, kv_heads, row_block):
    length, features = rows.shape
    width = columns.shape[1]
    q_width, kv_width = q_heads * HEAD_WIDTH, kv_heads * HEAD_WIDTH
    whole = lambda shape: pl.BlockSpec(shape, lambda i: (0, 0))
    part = lambda size: pl.BlockSpec((row_block, size), lambda i: (i, 0))
    return pl.pallas_call(
        functools.partial(project_kernel, q_heads, kv_heads),
        grid=(length // row_block,),
        out_shape=tuple(jax.ShapeDtypeStruct((length, n), jnp.bfloat16) for n in (q_width, kv_width, kv_width)),
        in_specs=[part(features), whole((1, features)), whole((features, width)),
                  whole((1, HEAD_WIDTH)), whole((1, HEAD_WIDTH)), part(HEAD_WIDTH), part(HEAD_WIDTH)],
        out_specs=(part(q_width), part(kv_width), part(kv_width)),
        cost_estimate=pl.CostEstimate(flops=2 * length * features * width, bytes_accessed=9_000_000, transcendentals=0),
        name="project_heads",
    )(rows, in_gain[None], columns, query_gain[None], key_gain[None], cosine, sine)


def attend_kernel(group, q_ref, k_ref, v_ref, o_ref):
    factor = HEAD_WIDTH ** (-0.5) * float(np.log2(np.e))
    for h in range(q_ref.shape[1] // HEAD_WIDTH):
        span = slice(h * HEAD_WIDTH, (h + 1) * HEAD_WIDTH)
        shared = slice(h // group * HEAD_WIDTH, (h // group + 1) * HEAD_WIDTH)
        scores = lax.dot_general(q_ref[:, span], k_ref[:, shared], (((1,), (1,)), ((), ())),
                                 preferred_element_type=jnp.float32)
        top = jnp.max(scores, axis=-1, keepdims=True)
        raised = jnp.exp2((scores - top) * factor)
        weights = (raised * (1.0 / jnp.sum(raised, axis=-1, keepdims=True))).astype(jnp.bfloat16)
        o_ref[:, span] = jnp.dot(
            weights, v_ref[:, shared], preferred_element_type=jnp.float32).astype(jnp.bfloat16)


def attend(q, k, v, q_heads, kv_heads, row_block):
    length = q.shape[0]
    block = pl.BlockSpec((row_block, q.shape[1]), lambda i: (i, 0))
    keys = pl.BlockSpec(k.shape, lambda i: (0, 0))
    return pl.pallas_call(
        functools.partial(attend_kernel, q_heads // kv_heads),
        grid=(length // row_block,),
        out_shape=jax.ShapeDtypeStruct(q.shape, jnp.bfloat16),
        in_specs=[block, keys, keys],
        out_specs=block,
        cost_estimate=pl.CostEstimate(flops=4 * length * length * q_heads * HEAD_WIDTH,
                                      bytes_accessed=3_000_000, transcendentals=length * length * q_heads),
        name="attend_heads",
    )(q, k, v)


def output_kernel(a_ref, head_ref, tail_ref, g_ref, o_ref, total):
    step = pl.program_id(0)
    split = head_ref.shape[1]

    @pl.when(step == 0)
    def _():
        total[...] = jnp.zeros_like(total)

    total[:, :split] += jnp.dot(a_ref[0], head_ref[...], preferred_element_type=jnp.float32)
    total[:, split:] += jnp.dot(a_ref[0], tail_ref[...], preferred_element_type=jnp.float32)

    @pl.when(step == pl.num_programs(0) - 1)
    def _():
        x = total[...]
        scale = lax.rsqrt(jnp.mean(x * x, axis=-1, keepdims=True) + EPS)
        o_ref[...] = (x * scale * g_ref[...]).astype(jnp.bfloat16)


def output(returned, out_head, out_tail, out_gain):
    parts, row_count, width = returned.shape
    features = out_gain.shape[0]
    split = out_head.shape[1]
    return pl.pallas_call(
        output_kernel,
        grid=(parts,),
        out_shape=jax.ShapeDtypeStruct((row_count, features), jnp.bfloat16),
        in_specs=[pl.BlockSpec((1, row_count, width), lambda s: (s, 0, 0)),
                  pl.BlockSpec((width, split), lambda s: (s, 0)),
                  pl.BlockSpec((width, features - split), lambda s: (s, 0)),
                  pl.BlockSpec((1, features), lambda s: (0, 0))],
        out_specs=pl.BlockSpec((row_count, features), lambda s: (0, 0)),
        scratch_shapes=[pltpu.VMEM((row_count, features), jnp.float32)],
        cost_estimate=pl.CostEstimate(flops=2 * row_count * features * width * parts,
                                      bytes_accessed=10_000_000, transcendentals=0),
        name="output_rows",
    )(returned, out_head, out_tail, out_gain[None])


def fused_kernel(
    chips, q_width, kv_width,
    x_in, wq_ref, wk_ref, wv_ref, wo_ref, ig_in, qg_in, kg_in, cos_ref, sin_ref,
    total,
    x_ref, ig_ref, qg_ref, kg_ref, xn, wkv, wqb, wob, q_buf, kv_buf, att, cosb, sinb,
    load_sem, tok_send, tok_recv, z_own, z_send, z_recv, y_send, y_recv, x_send, x_recv,
    kv_send, kv_recv, att_send, att_recv, p_send, p_recv, own_send, own_recv,
):
    sp, dp = lax.axis_index("sp"), lax.axis_index("dp")
    z, core = dp // 2, dp % 2
    yi, xi = sp // 2, sp % 2
    R, F = x_in.shape
    depth = wq_ref.shape[0]
    OD = wo_ref.shape[1]
    wide, narrow, rest = OD // 8, OD // 16, OD // 4
    shared = depth // 2
    width = 2 * q_width
    per = q_width // HEAD_WIDTH
    kv_per = kv_width // HEAD_WIDTH
    x_peer, y_peer = yi * 2 + (1 - xi), (1 - yi) * 2 + xi
    corner = (1 - yi) * 2 + (1 - xi)
    X = {"sp": x_peer, "dp": dp}
    Y = {"sp": y_peer, "dp": dp}
    PAIR = {"sp": sp, "dp": z * 2 + (1 - core)}
    others = chips - 1

    barrier = pltpu.get_barrier_semaphore()
    for peer in (X, Y, PAIR):
        pl.semaphore_signal(barrier, inc=1, device_id=peer, device_id_type=MESH)

    @pl.when(z < chips - 1)
    def _():
        pl.semaphore_signal(barrier, inc=1, device_id={"sp": sp, "dp": dp + 2}, device_id_type=MESH)

    @pl.when(z > 0)
    def _():
        pl.semaphore_signal(barrier, inc=1, device_id={"sp": sp, "dp": dp - 2}, device_id_type=MESH)

    loads = []

    def load(src, dst):
        copy = pltpu.make_async_copy(src, dst, load_sem.at[len(loads)])
        copy.start()
        loads.append(copy)

    mine = pl.ds(pl.multiple_of(dp * depth, depth), depth)
    load(x_in, x_ref)
    for j in range(2):
        at = pl.ds(pl.multiple_of((2 * xi + j) * kv_width, 128), kv_width)
        load(wk_ref.at[:, at], wkv.at[j, mine, pl.ds(0, kv_width)])
        load(wv_ref.at[:, at], wkv.at[j, mine, pl.ds(kv_width, kv_width)])
    for j in range(2):
        at = pl.ds(pl.multiple_of((2 * xi + j) * q_width, 128), q_width)
        load(wq_ref.at[:, at], wqb.at[j, mine])
    load(wo_ref, wob.at[mine])
    table = pl.ds(pl.multiple_of(yi * 2 * R, R), 2 * R)
    load(cos_ref.at[table], cosb)
    load(sin_ref.at[table], sinb)
    for source, target in ((ig_in, ig_ref), (qg_in, qg_ref), (kg_in, kg_ref)):
        load(source, target)

    in_chain = (z + others) // chips + (2 * others - z) // chips
    pl.semaphore_wait(barrier, 3 + in_chain)

    def send(make, sems, recvs, index, peer, make_dst=None):
        slot = index[0] if isinstance(index, tuple) else 0
        for src, dst in zip(make(), (make_dst or make)()):
            remote(src, dst, sems.at[slot], recvs.at[index], peer).start()

    def sent(ref, sems, slot):
        remote(ref, ref, sems.at[slot], p_recv.at[0], PAIR).wait_send()

    def arrived(ref, recvs, index):
        remote(ref, ref, p_send.at[0], recvs.at[index], PAIR).wait_recv()

    def rows(owner, of, start=0, size=depth):
        return pl.ds(pl.multiple_of((owner * 2 + of) * depth, depth) + start, size)

    def quarter(owner, of, who, a=0, b=2):
        broad = wob.at[rows(owner, of, a * depth // 2, (b - a) * depth // 2),
                       pl.ds(pl.multiple_of(who * wide, 128), wide)]
        slim = wob.at[rows(owner, of, a * shared // 2, (b - a) * shared // 2),
                      pl.ds(pl.multiple_of(4 * wide + who * narrow, 128), narrow)]
        return [broad, slim]

    def quarters(times, a=0, b=2):
        return wob.at[:times * (b - a) * (depth // 2 + shared // 4), :wide]

    def rests(times):
        return wob.at[:times * (2 * depth - shared), :rest]

    def block(t, owner, of, j=None):
        if t == 0:
            return [wkv.at[yi if j is None else j, rows(owner, of)]]
        if t == 1:
            return [wqb.at[yi if j is None else j, rows(owner, of)]]
        if t == 2:
            return quarter(owner, of, sp)
        return [wob.at[rows(owner, of), pl.ds(OD - rest, rest)],
                wob.at[rows(owner, of, shared, depth - shared), pl.ds(4 * wide, 4 * narrow)]]

    def bulk(t):
        if t == 0:
            return wkv.at[0, :depth]
        if t == 1:
            return wqb.at[0, :depth]
        return quarters(1) if t == 2 else rests(1)

    low = jnp.minimum(z, others - z)

    def owner_of(i):
        near = (i + 1) // 2
        paired = z - near if i % 2 else z + near
        alone = jnp.where(z > others - z, z - (i - low), z + (i - low))
        return jnp.where(i <= 2 * low, paired, alone)

    owners = [z] + [owner_of(i) for i in range(1, chips)]
    last_below = jnp.where(z == 0, 0, jnp.where(z <= others - z, 2 * z - 1, others))
    above = others - z
    last_above = jnp.where(above == 0, 0, jnp.where(above <= z, 2 * above, others))

    def start_q(up, part, when=None):
        ok = z < others if up else z > 0
        if when is not None:
            ok = jnp.logical_and(ok, when)

        @pl.when(ok)
        def _():
            ref = wqb.at[yi, rows(z, core, part * (depth // 2), depth // 2)]
            remote(ref, ref, z_own.at[1, int(up)], z_recv.at[1, z],
                   {"sp": sp, "dp": dp + (2 if up else -2)}).start()

    def start_own(t, up, now=None):
        ok = z < others if up else z > 0
        if now is not None:
            ok = jnp.logical_and(ok, (last_below if up else last_above) == now)

        @pl.when(ok)
        def _():
            for ref in block(t, z, core):
                remote(ref, ref, z_own.at[t, int(up)], z_recv.at[t, z],
                       {"sp": sp, "dp": dp + (2 if up else -2)}).start()

    def to_pair(kind, refs):
        group = {0: 0, 4: 0, 1: 1, 5: 2, 2: 3, 7: 4, 6: 5, 8: 6, 9: 6, 3: 7, 10: 8, 11: 9}[kind]
        for ref in refs:
            remote(ref, ref, p_send.at[group], p_recv.at[group], PAIR).start()

    def pair_refs():
        half = wqb.at[0, :F // 2]
        return ([wkv.at[0], half, half] + [quarters(others)] * 3
                + [quarters(others - 1), rests(others - 1), rests(1), quarters(1)])

    def pair_wait(group):
        ref = pair_refs()[group]
        remote(ref, ref, p_send.at[group], p_recv.at[group], PAIR).wait_recv()

    def relay_target(owner):
        step = jnp.where(owner < z, 1, -1)
        return jnp.logical_and(z + step >= 0, z + step < chips), {"sp": sp, "dp": dp + 2 * step}

    def from_z(t, i):
        owner = owners[i]
        arrived(bulk(t), z_recv, (t, owner))
        ok, peer = relay_target(owner)

        @pl.when(ok)
        def _():
            for ref in block(t, owner, core):
                remote(ref, ref, z_send.at[t, owner], z_recv.at[t, owner], peer).start()

        def make():
            return block(t, owner, core)

        if t == 0 or (t == 1 and i < others):
            send(make, y_send, y_recv, (t, owner), Y)
        if t == 2:
            send(make, x_send, x_recv, (0, owner), X)
        to_pair(10 if t == 3 and i == others else t, make())

    def share_y(t, i):
        owner = owners[i]
        send(lambda: block(t, owner, core), y_send, y_recv, (t, owner), Y)

    def from_y(t, i):
        owner = owners[i]
        arrived(bulk(t), y_recv, (t, owner))
        if t == 2:
            send(lambda: quarter(owner, core, y_peer, 0, 1), x_send, x_recv, (1, owner), X)
            to_pair(6, quarter(owner, core, y_peer))
        else:
            to_pair(4 + t, block(t, owner, core, 1 - yi))

    def from_x(i):
        owner = owners[i]
        arrived(bulk(2), x_recv, (0, owner))
        send(lambda: quarter(owner, core, x_peer, 1, 2), y_send, y_recv, (3, owner), Y)
        to_pair(7, quarter(owner, core, x_peer))

    def corner_x(i):
        owner = owners[i]
        arrived(quarters(1, 0, 1), x_recv, (1, owner))
        to_pair(11 if i == others else 8, quarter(owner, core, corner, 0, 1))

    def corner_y(i):
        owner = owners[i]
        arrived(quarters(1, 1, 2), y_recv, (3, owner))
        to_pair(11 if i == others else 9, quarter(owner, core, corner, 1, 2))

    for copy in loads[:5]:
        copy.wait()
    send(lambda: [x_ref], tok_send, tok_recv, 0, X, lambda: [xn.at[pl.ds(pl.multiple_of(xi * R, R), R)]])
    start_own(0, True)
    start_own(0, False)
    to_pair(0, block(0, z, core))
    to_pair(4, block(0, z, core, 1 - yi))
    for copy in loads[5:7]:
        copy.wait()
    start_q(True, 0)
    start_q(False, 0)
    to_pair(1, block(1, z, core))
    to_pair(5, block(1, z, core, 1 - yi))
    for copy in loads[7:]:
        copy.wait()
    remote(wob.at[mine], wob.at[mine], own_send.at[0], own_recv.at[0], PAIR).start()

    def normalize(values, start):
        x = values.astype(jnp.float32)
        scale = lax.rsqrt(jnp.mean(x * x, axis=-1, keepdims=True) + EPS)
        xn[pl.ds(pl.multiple_of(start, R), R)] = (x * scale * ig_ref[...]).astype(jnp.bfloat16)

    def stage_own(t, now):
        start_own(t, True, now)
        start_own(t, False, now)

    inner = low > 0
    outer = jnp.logical_not(inner)

    def only(when, *stages):
        @pl.when(when)
        def _():
            for stage in stages:
                stage()

    def columns_in(i):
        from_z(1, i)
        stage_own(2, i)

    def quarter_in(i):
        from_z(2, i)
        stage_own(3, i)

    normalize(x_ref[...], xi * R)
    for i in range(1, chips):
        from_z(0, i)
        if i == 1:
            start_q(True, 1)
            start_q(False, 1, outer)
            stage_own(2, 0)
            stage_own(3, 0)
        if i == min(2, others):
            start_q(False, 1, inner)
        if i > 1:
            from_y(0, i - 1)
            columns_in(i - 1)
        if i > 2:
            from_y(1, i - 2)
    only(inner, lambda: columns_in(others), *[functools.partial(quarter_in, i) for i in range(1, others)])

    lane = lax.broadcasted_iota(jnp.int32, (R, HEAD_WIDTH), 1)
    first = lane % (HEAD_WIDTH // 2) < HEAD_WIDTH // 4

    def finish(head, gain, cosine, sine):
        head = head * lax.rsqrt(jnp.mean(head * head, axis=-1, keepdims=True) + EPS) * gain
        other = jnp.where(first, pltpu.roll(head, HEAD_WIDTH - HEAD_WIDTH // 4, 1),
                          pltpu.roll(head, HEAD_WIDTH // 4, 1))
        return (head * cosine + other * sine).astype(jnp.bfloat16)

    def cut(values, h):
        return values[:, h * HEAD_WIDTH:(h + 1) * HEAD_WIDTH]

    if chips > 1:
        from_y(0, others)
    pair_wait(0)

    def keys_values(turn, who):
        local = pl.ds(pl.multiple_of(who * R, R), R)
        placed = pl.ds(pl.multiple_of((yi * 2 + who) * R, R), R)
        cosine, sine = cosb[local], sinb[local]
        for j in range(2):
            mixed = jnp.dot(xn[local], wkv[j], preferred_element_type=jnp.float32)
            for h in range(kv_per):
                kv_buf[j, placed, h * HEAD_WIDTH:(h + 1) * HEAD_WIDTH] = finish(
                    cut(mixed, h), kg_ref[...], cosine, sine)
            kv_buf[j, placed, kv_width:] = mixed[:, kv_width:].astype(jnp.bfloat16)
        send(lambda: [kv_buf.at[:, pl.ds(pl.multiple_of((yi * 2 + who) * R, R), R)]],
             kv_send, kv_recv, turn, Y)

    keys_values(0, xi)
    only(outer, lambda: columns_in(others))
    theirs = xn.at[pl.ds(pl.multiple_of((1 - xi) * R, R), R)]
    arrived(theirs, tok_recv, 0)
    normalize(theirs[...], (1 - xi) * R)
    keys_values(1, 1 - xi)

    def queries(j):
        @pl.loop(0, 2)
        def _(who):
            local = pl.ds(pl.multiple_of(who * R, R), R)
            cosine, sine = cosb[local], sinb[local]
            mixed = jnp.dot(xn[local], wqb[j], preferred_element_type=jnp.float32)
            for h in range(per):
                q_buf[j, local, h * HEAD_WIDTH:(h + 1) * HEAD_WIDTH] = finish(
                    cut(mixed, h), qg_ref[...], cosine, sine)

    share_y(1, others)
    only(inner, lambda: quarter_in(others))
    if chips > 2:
        from_y(1, others - 1)
    only(outer, lambda: quarter_in(1))
    share_y(2, 1)
    pair_wait(1)
    queries(yi)
    for i in range(min(2, others), 0, -1):
        only(inner, lambda i=i: from_z(3, i))
    for i in range(2, chips):
        only(outer, lambda i=i: quarter_in(i))
        share_y(2, i)
    from_x(1)
    for who in range(2):
        at = pl.ds(pl.multiple_of(((1 - yi) * 2 + (who + xi) % 2) * R, R), R)
        arrived(kv_buf.at[:, at], kv_recv, who)

    factor = HEAD_WIDTH ** (-0.5) * float(np.log2(np.e))
    couple = 2
    turns = per // couple

    def attend(mine, j, turn):
        who, place = (xi, xi) if mine else (1 - xi, 2)
        local = pl.ds(pl.multiple_of(who * R, R), R)
        for u in range(couple):
            head = turn * couple + u
            group = head // (per // kv_per) * HEAD_WIDTH
            at = slice(head * HEAD_WIDTH, (head + 1) * HEAD_WIDTH)
            scores = lax.dot_general(
                q_buf[j, local, at], kv_buf[j, :, group:group + HEAD_WIDTH], (((1,), (1,)), ((), ())),
                preferred_element_type=jnp.float32)
            top = jnp.max(scores, axis=-1, keepdims=True)
            raised = jnp.exp2((scores - top) * factor)
            weights = (raised * (1.0 / jnp.sum(raised, axis=-1, keepdims=True))).astype(jnp.bfloat16)
            values = kv_buf[j, :, kv_width + group:kv_width + group + HEAD_WIDTH]
            att[place, j, :, at] = jnp.dot(
                weights, values, preferred_element_type=jnp.float32).astype(jnp.bfloat16)

    def give(j, turn):
        at = pl.ds(turn * couple * HEAD_WIDTH, couple * HEAD_WIDTH)
        send(lambda: [att.at[2, j, :, at]], att_send, att_recv, 0, X, lambda: [att.at[xi, j, :, at]])

    early, late = [], []
    for i in range(2, others):
        early.append(lambda i=i: from_x(i))
    for i in range(max(2, others), chips):
        late.append(lambda i=i: from_x(i))
    for i in range(1, chips):
        if i > 1:
            late.append(lambda i=i: from_y(2, i))
        if i < others:
            late.append(lambda i=i: only(outer, lambda: from_z(3, i)))
    early += [lambda i=i: only(inner, lambda: from_z(3, i)) for i in range(3, chips)]
    for j, items in ((yi, early), (1 - yi, late)):
        if items is late:
            from_y(1, others)
            pair_wait(2)
            queries(j)
            from_y(2, 1)
        parts = [(own, turn) for own in (False, True) for turn in range(turns)]
        for n, (own, turn) in enumerate(parts):
            attend(own, j, turn)
            if not own:
                give(j, turn)
            for item in items[n * len(items) // len(parts):(n + 1) * len(items) // len(parts)]:
                item()

    def project(zones, mine):
        half = xi if mine else 1 - xi
        for at in zones:
            part = None if mine else total[:, at]
            for j in range(2):
                deep = pl.ds(pl.multiple_of((half * 2 + j) * q_width, q_width), q_width)
                term = jnp.dot(att[half, j], wob[deep, at], preferred_element_type=jnp.float32)
                part = term if part is None else part + term
            total[:, at] = part

    def zone(who):
        return pl.ds(pl.multiple_of(who * wide, 128), wide)

    def corners(i):
        corner_y(i)
        corner_x(i)

    arrived(wob.at[rows(z, 1 - core)], own_recv, 0)
    def project_late(at, first, stop):
        part = total[:, at] if first else None
        for owner in owners[first:stop]:
            deep = pl.ds(pl.multiple_of(owner * q_width, q_width), q_width)
            term = jnp.dot(att[owner // 2, owner % 2], wob[deep, at], preferred_element_type=jnp.float32)
            part = term if part is None else part + term
        total[:, at] = part

    pair_wait(3)
    pair_wait(4)
    project([zone(sp), zone(x_peer)], True)
    corners(1)
    arrived(att.at[1 - xi], att_recv, 0)
    project([zone(sp), zone(x_peer)], False)
    for i in range(2, others):
        corners(i)
    pair_wait(5)
    project([zone(y_peer)], True)
    project([zone(y_peer)], False)
    pair_wait(7)
    corners(others)
    only(outer, lambda: from_z(3, others))
    project_late(slice(OD - rest, OD), 0, others)
    pair_wait(6)
    project_late(slice(4 * wide, OD - rest), 0, others)
    project_late(zone(corner), 0, others)
    pair_wait(9)
    project_late(zone(corner), others, chips)
    pair_wait(8)
    project_late(slice(4 * wide, OD), others, chips)

    count = others * depth
    sent(x_ref, tok_send, 0)
    sent(wkv.at[0, :count], y_send, 0)
    sent(wqb.at[0, :count], y_send, 1)
    sent(quarters(others), y_send, 2)
    sent(quarters(others, 1, 2), y_send, 3)
    sent(quarters(others), x_send, 0)
    sent(quarters(others, 0, 1), x_send, 1)
    sent(kv_buf.at[:, :2 * R], kv_send, 0)
    sent(att.at[2], att_send, 0)
    for group, ref in enumerate(pair_refs()):
        sent(ref, p_send, group)
    sent(wob.at[mine], own_send, 0)
    for t in range(4):
        @pl.when(z < others)
        def _():
            ref = bulk(t)
            remote(ref, ref, z_own.at[t, 1], z_recv.at[t, z], PAIR).wait_send()

        @pl.when(z > 0)
        def _():
            ref = bulk(t)
            remote(ref, ref, z_own.at[t, 0], z_recv.at[t, z], PAIR).wait_send()

        for i in range(1, chips):
            owner = owners[i]
            ok, peer = relay_target(owner)

            @pl.when(ok)
            def _():
                ref = bulk(t)
                remote(ref, ref, z_send.at[t, owner], z_recv.at[t, owner], peer).wait_send()


def rows_kernel(total, gain, o_ref, out, sem):
    R = total.shape[0]
    chunk = R // 4
    for n in range(4):
        at = pl.ds(n * chunk, chunk)
        x = total[at]
        scale = lax.rsqrt(jnp.mean(x * x, axis=-1, keepdims=True) + EPS)
        out[at] = (x * scale * gain[...]).astype(jnp.bfloat16)
        pltpu.make_async_copy(out.at[at], o_ref.at[at], sem).start()
    pltpu.make_async_copy(out, o_ref, sem).wait()


def finish_rows(total, gain):
    vmem = pl.BlockSpec(memory_space=pltpu.VMEM)
    return pl.pallas_call(
        rows_kernel,
        out_shape=jax.ShapeDtypeStruct(total.shape, jnp.bfloat16),
        in_specs=[vmem, vmem],
        out_specs=ANY,
        scratch_shapes=[pltpu.VMEM(total.shape, jnp.bfloat16), pltpu.SemaphoreType.DMA],
        compiler_params=pltpu.CompilerParams(vmem_limit_bytes=8 * 1024 * 1024),
        cost_estimate=pl.CostEstimate(flops=4_000_000, bytes_accessed=2_000_000, transcendentals=0),
        name="finish_rows",
    )(total, gain[None])


def fused(sequence, in_gain, query_weight, key_weight, value_matrix, query_gain, key_gain,
          out_weight, out_gain, cosine, sine, chips):
    row_count, features = sequence.shape
    q_width, kv_width = query_weight.shape[1] // 4, key_weight.shape[1] // 4
    columns = out_weight.shape[1]
    dma = pltpu.SemaphoreType.DMA
    bf16, f32 = jnp.bfloat16, jnp.float32
    total = pl.pallas_call(
        functools.partial(fused_kernel, chips, q_width, kv_width),
        out_shape=pltpu.VMEM((row_count, columns), f32),
        in_specs=[pl.BlockSpec(memory_space=pltpu.HBM)] * 10,
        out_specs=pl.BlockSpec(memory_space=pltpu.VMEM),
        scratch_shapes=[
            pltpu.VMEM((row_count, features), bf16),
            pltpu.VMEM((1, features), f32),
            pltpu.VMEM((1, HEAD_WIDTH), f32),
            pltpu.VMEM((1, HEAD_WIDTH), f32),
            pltpu.VMEM((2 * row_count, features), bf16),
            pltpu.VMEM((2, features, 2 * kv_width), bf16),
            pltpu.VMEM((2, features, q_width), bf16),
            pltpu.VMEM((out_weight.shape[0] * chips * 2, columns), bf16),
            pltpu.VMEM((2, 2 * row_count, q_width), bf16),
            pltpu.VMEM((2, 4 * row_count, 2 * kv_width), bf16),
            pltpu.VMEM((3, 2, row_count, q_width), bf16),
            pltpu.VMEM((2 * row_count, HEAD_WIDTH), f32),
            pltpu.VMEM((2 * row_count, HEAD_WIDTH), f32),
            dma((14,)), dma((1,)), dma((1,)), dma((4, 2)), dma((4, chips)), dma((4, chips)),
            dma((4,)), dma((4, chips)), dma((2,)), dma((2, chips)),
            dma((1,)), dma((2,)), dma((1,)), dma((1,)), dma((10,)), dma((10,)), dma((1,)), dma((1,)),
        ],
        compiler_params=pltpu.CompilerParams(
            collective_id=0, has_side_effects=True, vmem_limit_bytes=56 * 1024 * 1024),
        cost_estimate=pl.CostEstimate(flops=10_000_000_000, bytes_accessed=10_000_000, transcendentals=0),
        name="attention_layer",
    )(sequence, query_weight, key_weight, value_matrix, out_weight, in_gain[None], query_gain[None],
      key_gain[None], cosine, sine)
    return finish_rows(total, out_gain)


def rotation(length):
    quarter = HEAD_WIDTH // 4
    inverse_freq = (THETA ** (-np.arange(quarter, dtype=np.float32) / quarter)).astype(np.float32)

    def table(count):
        angle = (np.arange(count, dtype=np.float32)[:, None] * inverse_freq[None, :]).astype(np.float64)
        cosine, sine = np.cos(angle), np.sin(angle)
        return (np.concatenate([cosine, cosine], 1).astype(np.float32),
                np.concatenate([-sine, sine], 1).astype(np.float32))

    rows = -(-length // GRID_W)
    row_tables, col_tables = table(rows), table(GRID_W)
    half = HEAD_WIDTH // 2
    out = []
    for row, col in zip(row_tables, col_tables):
        row = np.broadcast_to(row[:, None, :], (rows, GRID_W, half))
        col = np.broadcast_to(col[None, :, :], (rows, GRID_W, half))
        full = np.concatenate([row, col], -1).reshape(rows * GRID_W, HEAD_WIDTH)
        out.append(jnp.asarray(full[:length]))
    return out


def on_device(parts, groups, tokens, in_gain, query_weight, key_weight, value_matrix,
              query_gain, key_gain, out_weight, out_gain):
    sequence = tokens[0]
    row_count = sequence.shape[0]
    q_heads = QUERY_HEAD_COUNT // parts
    kv_heads = max(1, KEY_VALUE_HEADS // parts)
    per_group = QUERY_HEAD_COUNT // KEY_VALUE_HEADS
    cosine, sine = rotation(parts * row_count)
    if parts == 4 and groups == 8:
        return fused(sequence, in_gain, query_weight, key_weight, value_matrix, query_gain, key_gain,
                     out_weight, out_gain, cosine, sine, groups // 2)[None]
    rows, columns, out_head, own_tail = gather(
        sequence, query_weight, key_weight, value_matrix, out_weight, parts, groups // 2,
        q_heads * HEAD_WIDTH, kv_heads * HEAD_WIDTH, lambda sp: sp * q_heads // per_group)
    out_tail = lax.all_gather(own_tail, "dp", axis=0, tiled=True)
    q, k, v = project(rows, in_gain, columns, query_gain, key_gain, cosine, sine, q_heads, kv_heads, row_count)
    attended = attend(q, k, v, q_heads, kv_heads, row_count)
    returned = exchange(attended, parts)
    return output(returned, out_head, out_tail, out_gain)[None]


def solution(mesh):
    placed = (P("dp", "sp", None), P(), P("dp", None), P("dp", None), P("dp", None),
              P(), P(), P("dp", None), P())
    return jax.shard_map(
        functools.partial(on_device, mesh.shape["sp"], mesh.shape["dp"]),
        mesh=mesh, in_specs=placed, out_specs=P("dp", "sp", None), check_vma=False,
    )
```
